256 devices in a mesh: ep: 128 (over z, y, x), tp: 2 (over core).
Axes of the slice: x: 4, y: 4, z: 8, core: 2. Of those that a mesh axis runs over, the one named last changes fastest.
Arguments:
- tokens: bfloat16 [8192, 1024], P('ep', 'tp'), may hold values from -6 to 6
- norm_gain: float32 [1024], P('tp'), may hold values from 0.1 to 1.9
- routing: int32 [8192, 2], P('ep'), may hold values from 0 to 255, as said below
- route_weight: float32 [8192, 2], P('ep'), may hold values from 0.25 to 1
- w_gate: bfloat16 [256, 1024, 512], P('ep', None, 'tp'), may hold values from -0.1875 to 0.1875
- w_up: bfloat16 [256, 1024, 512], P('ep', None, 'tp'), may hold values from -0.1875 to 0.1875
- w_down: bfloat16 [256, 512, 1024], P('ep', None, 'tp'), may hold values from -0.25 to 0.25
Outputs:
- mixed: bfloat16 [8192, 1024], P('ep', 'tp')
The draws below stay inside these ranges and needn't reach their ends.
Inputs may be any that keep to these rules, and one draw needn't show every extreme that they name: `routing`: each row names 2 different experts, all in the same group of 8 consecutive expert numbers. Among the rows of one device (aligned blocks of 64 rows) no expert is named more than 8 times, and in every block some expert is named exactly 8 times.
All inputs are finite; a program needn't handle non-finite values.
Results may differ from the reference program's by a relative error of at most 0.0015.
Values may be sent and summed in bfloat16 or wider, within the bound.
A program may use at most 64 MiB of HBM per device.

```python
import jax
import jax.numpy as jnp
from jax import lax

D = 1024
FFE = 512
TOP_K = 2
GROUP_EXP = 8
EXP_DEV = 2
CAP = 8
TOK_DEV = 64
EXPERTS = 256
TOKENS = 8192


def route_table(key):
    blocks = TOKENS // TOK_DEV
    groups = EXPERTS // GROUP_EXP
    semi_cluster = GROUP_EXP // 2
    opening_tally = EXPERTS // 2
    cell_count = TOK_DEV // CAP
    pop_key = jax.random.fold_in(key, 11)
    group_scores = jax.random.randint(pop_key, (groups,), 0, 1 << 20) * groups + jnp.arange(groups)
    ranking = jnp.argsort(jnp.argsort(group_scores))
    favoured_specialist = ranking < max(1, groups // 4)
    extra_cluster = jnp.where(favoured_specialist, 400, 0)
    base_key = jax.random.fold_in(key, 23)

    def one_block(block_id):
        block_key = jax.random.fold_in(base_key, block_id)
        perm_key, rating_seed, seat_key, flip_key = jax.random.split(block_key, 4)
        raw = jax.random.randint(perm_key, (groups, GROUP_EXP), 0, 1 << 20) * GROUP_EXP + jnp.arange(GROUP_EXP)[None, :]
        local_perm = jnp.argsort(raw, axis=1)
        pair_table = (jnp.arange(groups)[:, None] * GROUP_EXP + local_perm).reshape(opening_tally, 2)
        position = jnp.argsort(pair_table.reshape(-1))
        slot_of = position // 2
        forward = (block_id + blocks // 2) % blocks * EXP_DEV
        previous = (block_id + blocks - 1) % blocks * EXP_DEV
        opening_labels = jnp.arange(opening_tally)
        affinity_grades = jax.random.randint(rating_seed, (opening_tally,), 0, 1024) + extra_cluster[opening_labels // semi_cluster]
        affinity_grades = affinity_grades + 8192 * (opening_labels == slot_of[forward]) + 8192 * (opening_labels == slot_of[previous])
        affinity_grades = affinity_grades * opening_tally + opening_labels
        unused, chosen = lax.top_k(affinity_grades, cell_count)
        seating = jax.random.permutation(seat_key, TOK_DEV)
        cell_of = seating // CAP
        pair_ids = pair_table[chosen[cell_of]]
        flipped = jax.random.randint(flip_key, (TOK_DEV,), 0, 2)
        first_pick = jnp.where(flipped == 1, pair_ids[:, 1], pair_ids[:, 0])
        second_pick = jnp.where(flipped == 1, pair_ids[:, 0], pair_ids[:, 1])
        return jnp.stack([first_pick, second_pick], axis=1)
    table = jax.vmap(one_block)(jnp.arange(blocks))
    return table.reshape(TOKENS, 2)


def draw_routing(key, part):
    return route_table(key).astype(jnp.int32)


def block_levels(key, shape, pieces, low, top_value):
    loudness, own = 1.0, jax.random.fold_in(key, 6)
    for dim, blocks in pieces:
        steps = jnp.exp(jax.random.uniform(jax.random.fold_in(own, dim), (blocks,), jnp.float32, low / len(pieces), top_value / len(pieces)))
        loudness = loudness * jnp.repeat(steps, shape[dim] // blocks).reshape([-1 if axis == dim else 1 for axis in range(len(shape))])
    return loudness


def scatter_about(stream_key, extent, width, reach, pieces=(), kind=jnp.bfloat16):
    loudness = block_levels(stream_key, extent, pieces, -0.22, 0.18) if pieces else 1.0
    array = jax.random.normal(stream_key, extent, jnp.float32) * width * loudness
    return jnp.minimum(jnp.maximum(array, -reach), reach).astype(kind)


def setup_inputs(seed: int = 0) -> dict:
    key_of = jax.random.split(jax.random.key(seed), 8)
    return {
        "tokens": scatter_about(key_of[0], (TOKENS, D), 1.0, 6.0, ((0, 128), (1, 2))),
        "norm_gain": jnp.clip(1.0 + 0.18 * jax.random.normal(key_of[1], (D,), jnp.float32), 0.1, 1.9),
        "routing": draw_routing(jax.random.fold_in(key_of[7], 71), 0),
        "route_weight": jnp.clip(0.25 + 0.75 * jax.random.uniform(key_of[3], (TOKENS, TOP_K), jnp.float32) ** block_levels(key_of[3], (TOKENS, TOP_K), ((0, 128),), -0.2, 0.2), 0.25, 1.0),
        "w_gate": scatter_about(key_of[4], (EXPERTS, D, FFE), D ** -0.5, 0.1875, ((0, 128), (2, 2))),
        "w_up": scatter_about(key_of[5], (EXPERTS, D, FFE), D ** -0.5, 0.1875, ((0, 128), (2, 2))),
        "w_down": scatter_about(key_of[6], (EXPERTS, FFE, D), FFE ** -0.5, 0.25, ((0, 128), (2, 2))),
    }


epsilon = 1e-06

def reference(tokens, norm_gain, routing, route_weight, w_gate, w_up, w_down):
    row_span = 32
    float_rows = tokens.astype(jnp.float32)
    scale = lax.rsqrt(lax.optimization_barrier(jnp.mean(float_rows * float_rows, axis=1, keepdims=True)) + epsilon)
    normed = (float_rows * scale * norm_gain[None, :]).astype(jnp.bfloat16)
    count = TOKENS * TOP_K
    flat_expert = routing.reshape(-1).astype(jnp.int32)
    flat_token = (jnp.arange(count) // TOP_K).astype(jnp.int32)
    flat_weight = route_weight.reshape(-1)
    sorting = jnp.argsort(flat_expert, stable=True).astype(jnp.int32)
    sorted_expert = flat_expert[sorting]
    counts = jnp.zeros((EXPERTS,), jnp.int32).at[flat_expert].add(1)
    starts = (jnp.cumsum(counts) - counts).astype(jnp.int32)
    padded = ((counts + row_span - 1) // row_span * row_span).astype(jnp.int32)
    pad_end = jnp.cumsum(padded).astype(jnp.int32)
    pad_start = (pad_end - padded).astype(jnp.int32)
    target = (pad_start[sorted_expert] + jnp.arange(count).astype(jnp.int32) - starts[sorted_expert]).astype(jnp.int32)
    block_count = -(-count // row_span) + EXPERTS
    row_total = block_count * row_span
    buffer = jnp.zeros((row_total, D), jnp.bfloat16).at[target].set(normed[flat_token[sorting]])
    block_expert = jnp.searchsorted(pad_end, (jnp.arange(block_count) * row_span).astype(jnp.int32), side='right')
    block_expert = jnp.minimum(block_expert.astype(jnp.int32), EXPERTS - 1).astype(jnp.int32)

    def run_block(inputs):
        block_rows, expert = inputs
        gate_acc = jnp.dot(block_rows, w_gate[expert], preferred_element_type=jnp.float32)
        up_acc = jnp.dot(block_rows, w_up[expert], preferred_element_type=jnp.float32)
        hidden = (jax.nn.silu(gate_acc) * up_acc).astype(jnp.bfloat16)
        return jnp.dot(hidden, w_down[expert], preferred_element_type=jnp.float32).astype(jnp.bfloat16)
    result = lax.map(run_block, (buffer.reshape(block_count, row_span, D), block_expert)).reshape(row_total, D)
    picked = result[target].astype(jnp.float32) * flat_weight[sorting][:, None]
    combined = jax.ops.segment_sum(picked, flat_token[sorting], num_segments=TOKENS)
    return combined.astype(jnp.bfloat16)
```

```python
import functools

import jax
import jax.numpy as jnp
from jax import lax
from jax.experimental import pallas as pl
from jax.experimental.pallas import tpu as pltpu
from jax.sharding import PartitionSpec as P

CAP = 8
EPSILON = 1e-06
MESH = pl.DeviceIdType.MESH

Z, Y, X = 8, 4, 4
EXPERTS = 2 * X
SLOTS = EXPERTS * CAP // 2
OFFSETS = Z * Y
STEPS = (0, 1, 7, 2, 6, 3, 5, 4)
ROUNDS = ((0, 1), (1, 3), (3, 5), (5, 7), (7, 8))
SEND_ORDER = (0, 1, 2, 3, 4)
ORDER = (
    "A0", "A1", "F0", "A2", "F1", "C0", "A3", "F2", "C1", "A4", "F3", "C2", "F4", "C3", "C4",
    "H0", "H1", "H2", "H3", "H4",
)


def kernel(
    tok_hbm, gain_hbm, routing_hbm, weight_hbm, wg_hbm, wu_hbm, wd_hbm, out_ref,
    tok, routing, weight, gains, wg, wu, wd, give_g, give_u, give_d,
    meta_s, meta_r, pick_home, send_1, recv_1, send_2, recv_2, send_3, recv_3, send_4, recv_4,
    in_sem, own_sem, give_sem, far_send, far_recv, s_sem, meta_sem, sem_1, sem_2, sem_3, sem_4,
):
    me, core = lax.axis_index("ep"), lax.axis_index("tp")
    other = 1 - core
    z, y, x = me // (Y * X), me // X % Y, me % X
    tokens, half = tok.shape

    def plane(step, dy, sign):
        if sign > 0:
            return ((z + step) % Z * Y + (y + dy) % Y) * X + x
        return ((z + Z - step) % Z * Y + (y + Y - dy) % Y) * X + x

    def line(dx, sign):
        return me - x + (x + (dx if sign > 0 else X - dx)) % X

    stores = ((wg_hbm, wg, give_g), (wu_hbm, wu, give_u), (wd_hbm, wd, give_d))
    inputs = ((routing_hbm, routing), (weight_hbm, weight), (tok_hbm, tok), (gain_hbm, gains.at[core]))
    inputs = [pltpu.make_async_copy(src, dst, in_sem.at[i]) for i, (src, dst) in enumerate(inputs)]
    own = [
        pltpu.make_async_copy(src.at[core], dst.at[core], own_sem.at[i])
        for i, (src, dst, _) in enumerate(stores)
    ]
    give = [
        pltpu.make_async_copy(src.at[other], stage, give_sem.at[i])
        for i, (src, _, stage) in enumerate(stores)
    ]
    for copy in inputs:
        copy.start()

    barrier = pltpu.get_barrier_semaphore()
    greeted = 0
    for step in STEPS:
        for dy in range(Y):
            if step or dy:
                pl.semaphore_signal(barrier, inc=1, device_id=(plane(step, dy, 1), core), device_id_type=MESH)
                greeted += 1
    for dx in range(X):
        for c in range(2):
            if dx:
                pl.semaphore_signal(barrier, inc=1, device_id=(line(dx, 1), c), device_id_type=MESH)
                greeted += 1
    pl.semaphore_signal(barrier, inc=1, device_id=(me, other), device_id_type=MESH)
    greeted += 1
    for copy in give + own:
        copy.start()

    row = lax.broadcasted_iota(jnp.int32, (tokens, tokens), 0)
    col = lax.broadcasted_iota(jnp.int32, (tokens, tokens), 1)
    before = (row < col).astype(jnp.float32).astype(jnp.bfloat16)
    names = lax.broadcasted_iota(jnp.int32, (OFFSETS * EXPERTS, tokens), 0)
    inputs[0].wait()
    picks = [routing[k:k + 1, :] for k in range(2)]
    group = picks[0] // EXPERTS
    dz = (group // Y - z + Z) % Z
    dy = (group % Y - y + Y) % Y
    place = jnp.where(dz <= Z // 2, jnp.maximum(2 * dz - 1, 0), 2 * (Z - dz)) * Y + dy
    hot = [(picks[k] == names).astype(jnp.float32) for k in range(2)]
    hot_place = (place == names[:OFFSETS]).astype(jnp.float32)
    both = jnp.concatenate([hot[0] + hot[1], hot_place], axis=0).astype(jnp.bfloat16)
    earlier = jnp.dot(both, before, preferred_element_type=jnp.float32)
    slot = jnp.sum(earlier[OFFSETS * EXPERTS:] * hot_place, axis=0, keepdims=True)
    spot = place.astype(jnp.float32) * SLOTS + slot
    codes = [
        (picks[k] % EXPERTS * CAP + 1).astype(jnp.float32)
        + jnp.sum(earlier[:OFFSETS * EXPERTS] * hot[k], axis=0, keepdims=True)
        for k in range(2)
    ]
    inputs[1].wait()
    rows = [spot] + codes + [weight[k:k + 1, :] for k in range(2)] + [jnp.zeros_like(spot)] * 3
    columns = jnp.transpose(jnp.concatenate(rows, axis=0))
    slots = OFFSETS * SLOTS
    lanes = lax.broadcasted_iota(jnp.int32, (tokens, slots), 1)
    at_home = lanes == columns[:, 0:1].astype(jnp.int32)
    pick_home[...] = at_home.astype(jnp.float32).astype(jnp.bfloat16)
    for q in range(4):
        values = jnp.sum(jnp.where(at_home, columns[:, q + 1:q + 2], 0.0), axis=0, keepdims=True)
        for p in range(Z):
            meta_s[p, q:q + 1, :] = values[:, p * Y * SLOTS:(p + 1) * Y * SLOTS]
    spread = lax.broadcasted_iota(jnp.int32, (slots, tokens), 0) == spot.astype(jnp.int32)
    spread = spread.astype(jnp.float32).astype(jnp.bfloat16)
    inputs[2].wait()
    outgoing = jnp.dot(spread, tok[...], preferred_element_type=jnp.float32)
    send_1[...] = outgoing.astype(jnp.bfloat16).reshape(OFFSETS, SLOTS, half)
    inputs[3].wait()

    pl.semaphore_wait(barrier, greeted)

    def remote(src, dst, send, recv, peer, c):
        return pltpu.make_async_remote_copy(
            src_ref=src, dst_ref=dst, send_sem=send, recv_sem=recv,
            device_id=(peer, c), device_id_type=MESH,
        )

    pltpu.make_async_copy(meta_s.at[0], meta_r.at[0], meta_sem.at[0]).start()
    pltpu.make_async_copy(send_1.at[0], recv_1.at[0], sem_1.at[0]).start()
    for r in SEND_ORDER:
        for dy in range(Y):
            for p in range(*ROUNDS[r]):
                if p or dy:
                    o, peer = p * Y + dy, plane(STEPS[p], dy, 1)
                    remote(meta_s.at[p], meta_r.at[o], s_sem.at[0], meta_sem.at[r], peer, core).start()
                    remote(send_1.at[o], recv_1.at[o], s_sem.at[1], sem_1.at[r], peer, core).start()

    gain_copy = remote(gains.at[core], gains.at[core], far_send.at[3], far_recv.at[3], me, other)
    gain_copy.start()
    for copy in give:
        copy.wait()
    far = [
        remote(stage, dst.at[core], far_send.at[i], far_recv.at[i], me, other)
        for i, (_, dst, stage) in enumerate(stores)
    ]
    for copy in far:
        copy.start()

    def arrived(ref, sem):
        pltpu.make_async_copy(ref, ref, sem).wait()

    def codes_of(r):
        parts = []
        segment = lax.broadcasted_iota(jnp.int32, (4, Y * SLOTS), 1) // SLOTS
        for p in range(*ROUNDS[r]):
            part = jnp.zeros((4, Y * SLOTS), jnp.float32)
            for dy in range(Y):
                part = jnp.where(segment == dy, meta_r[p * Y + dy], part)
            parts.append(part)
        return parts

    def full(code, block, blocks):
        code = code.astype(jnp.int32) - 1
        return (code >> 3) * (blocks * CAP) + block * CAP + (code & 7)

    def extent(r):
        first, last = ROUNDS[r]
        return first * Y, (last - first) * Y

    def step_a(r):
        first, blocks = extent(r)
        here = pl.ds(first, blocks)
        arrived(meta_r.at[here], meta_sem.at[r])
        table = codes_of(r)
        table = jnp.concatenate(table, axis=1) if len(table) > 1 else table[0]
        block = lax.broadcasted_iota(jnp.int32, (1, blocks * SLOTS), 1) // SLOTS
        places = lax.broadcasted_iota(jnp.int32, (EXPERTS * blocks * CAP, blocks * SLOTS), 0)
        hit = [places == full(table[k:k + 1, :], block, blocks) for k in range(2)]
        pick = (hit[0] | hit[1]).astype(jnp.float32).astype(jnp.bfloat16)
        arrived(recv_1.at[here], sem_1.at[r])
        source = recv_1[first:first + blocks].reshape(blocks * SLOTS, half)
        lined = jnp.dot(pick, source, preferred_element_type=jnp.float32).astype(jnp.bfloat16)
        at = pl.ds(first * CAP, blocks * CAP)
        send_2[:, first * CAP:(first + blocks) * CAP, :] = lined.reshape(EXPERTS, blocks * CAP, half)
        for dx in (2, 1, 3):
            peer = line(dx, 1)
            for c in range(2):
                remote(
                    send_2.at[(x + dx) % X * 2 + c, at], recv_2.at[dx, core, at], s_sem.at[2], sem_2.at[r], peer, c
                ).start()
        remote(send_2.at[x * 2 + other, at], recv_2.at[0, core, at], s_sem.at[2], sem_2.at[r], me, other).start()
        pltpu.make_async_copy(send_2.at[x * 2 + core, at], recv_2.at[0, core, at], sem_2.at[r]).start()

    ready = []

    def step_f(r):
        first, blocks = extent(r)
        count = blocks * CAP
        at = pl.ds(first * CAP, count)
        arrived(recv_2.at[:, :, at], sem_2.at[r])
        if not ready:
            gain_copy.wait()
        parts = [
            recv_2[:, h, first * CAP:first * CAP + count, :].astype(jnp.float32).reshape(X * count, half)
            for h in range(2)
        ]
        squares = sum(jnp.sum(p * p, axis=1, keepdims=True) for p in parts)
        scale = lax.rsqrt(squares / (2 * half) + EPSILON)
        normed = jnp.concatenate(
            [(p * scale * gains[h]).astype(jnp.bfloat16) for h, p in enumerate(parts)], axis=1
        )
        if not ready:
            for copy in own + far[:2]:
                copy.wait()
        hidden = []
        for h in range(2):
            gate = jnp.dot(normed, wg[h], preferred_element_type=jnp.float32)
            up = jnp.dot(normed, wu[h], preferred_element_type=jnp.float32)
            hidden.append((jax.nn.silu(gate) * up).astype(jnp.bfloat16))
        hidden = jnp.concatenate(hidden, axis=1)
        if not ready:
            far[2].wait()
            ready.append(True)
        for f in range(2):
            result = jnp.dot(hidden, wd[f], preferred_element_type=jnp.float32).astype(jnp.bfloat16)
            send_3[:, f, first * CAP:first * CAP + count, :] = result.reshape(X, count, half)
        mine = x * 2 + core
        for dx in (2, 1, 3):
            peer = line(dx, -1)
            for c in range(2):
                remote(
                    send_3.at[dx, c, at], recv_3.at[mine, at], s_sem.at[3], sem_3.at[r], peer, c
                ).start()
        remote(send_3.at[0, other, at], recv_3.at[mine, at], s_sem.at[3], sem_3.at[r], me, other).start()
        pltpu.make_async_copy(send_3.at[0, core, at], recv_3.at[mine, at], sem_3.at[r]).start()

    def step_c(r):
        first, blocks = extent(r)
        at = pl.ds(first * CAP, blocks * CAP)
        table = [jnp.transpose(jnp.concatenate([t, jnp.zeros_like(t)], axis=0)) for t in codes_of(r)]
        table = jnp.concatenate(table, axis=0) if len(table) > 1 else table[0]
        block = lax.broadcasted_iota(jnp.int32, (blocks * SLOTS, 1), 0) // SLOTS
        places = lax.broadcasted_iota(jnp.int32, (blocks * SLOTS, EXPERTS * blocks * CAP), 1)
        take = [
            (places == full(table[:, k:k + 1], block, blocks)).astype(jnp.float32).astype(jnp.bfloat16)
            for k in range(2)
        ]
        arrived(recv_3.at[:, at], sem_3.at[r])
        source = recv_3[:, first * CAP:(first + blocks) * CAP, :].reshape(EXPERTS * blocks * CAP, half)
        total = 0.0
        for k in range(2):
            total = total + table[:, 2 + k:3 + k] * jnp.dot(take[k], source, preferred_element_type=jnp.float32)
        send_4[first:first + blocks] = total.astype(jnp.bfloat16).reshape(blocks, SLOTS, half)
        for dy in range(Y):
            for p in range(*ROUNDS[r]):
                o = p * Y + dy
                if o:
                    remote(
                        send_4.at[o], recv_4.at[o], s_sem.at[4], sem_4.at[r], plane(STEPS[p], dy, -1), core
                    ).start()
                else:
                    pltpu.make_async_copy(send_4.at[0], recv_4.at[0], sem_4.at[r]).start()

    sums = []

    def step_h(r):
        first, blocks = extent(r)
        here = pl.ds(first, blocks)
        arrived(recv_4.at[here], sem_4.at[r])
        source = recv_4[first:first + blocks].reshape(blocks * SLOTS, half)
        take = pick_home[:, first * SLOTS:(first + blocks) * SLOTS]
        sums.append(jnp.dot(take, source, preferred_element_type=jnp.float32))

    step_of = {"A": step_a, "F": step_f, "C": step_c, "H": step_h}
    for name in ORDER:
        step_of[name[0]](int(name[1]))
    out_ref[...] = sum(sums).astype(jnp.bfloat16)

    arrived(meta_r.at[pl.ds(1, OFFSETS - 1)], s_sem.at[0])
    arrived(send_1.at[pl.ds(1, OFFSETS - 1)], s_sem.at[1])
    arrived(send_2.at[pl.ds(1, EXPERTS - 1)], s_sem.at[2])
    arrived(send_2.at[pl.ds(1, EXPERTS - 1)], s_sem.at[3])
    arrived(send_4.at[pl.ds(1, OFFSETS - 1)], s_sem.at[4])


def solution(mesh):
    assert mesh.shape["ep"] == Z * Y * X and mesh.shape["tp"] == 2

    def local(tokens, norm_gain, routing, route_weight, w_gate, w_up, w_down):
        rows, half = tokens.shape
        vmem = pl.BlockSpec(memory_space=pltpu.VMEM)
        far = pl.BlockSpec(memory_space=pl.ANY)
        dma = pltpu.SemaphoreType.DMA
        bf16, f32 = jnp.bfloat16, jnp.float32
        blocks = OFFSETS * CAP
        rounds = dma((len(ROUNDS),))
        return pl.pallas_call(
            kernel,
            out_shape=pltpu.VMEM((rows, half), bf16),
            in_specs=[far] * 7,
            out_specs=vmem,
            scratch_shapes=[
                pltpu.VMEM((rows, half), bf16),
                pltpu.VMEM((2, rows), jnp.int32),
                pltpu.VMEM((2, rows), f32),
                pltpu.VMEM((2, 1, half), f32),
                pltpu.VMEM(w_gate.shape, bf16),
                pltpu.VMEM(w_up.shape, bf16),
                pltpu.VMEM(w_down.shape, bf16),
                pltpu.VMEM(w_gate.shape[1:], bf16),
                pltpu.VMEM(w_up.shape[1:], bf16),
                pltpu.VMEM(w_down.shape[1:], bf16),
                pltpu.VMEM((Z, 4, Y * SLOTS), f32),
                pltpu.VMEM((OFFSETS, 4, Y * SLOTS), f32),
                pltpu.VMEM((rows, OFFSETS * SLOTS), bf16),
                pltpu.VMEM((OFFSETS, SLOTS, half), bf16),
                pltpu.VMEM((OFFSETS, SLOTS, half), bf16),
                pltpu.VMEM((EXPERTS, blocks, half), bf16),
                pltpu.VMEM((X, 2, blocks, half), bf16),
                pltpu.VMEM((X, 2, blocks, half), bf16),
                pltpu.VMEM((EXPERTS, blocks, half), bf16),
                pltpu.VMEM((OFFSETS, SLOTS, half), bf16),
                pltpu.VMEM((OFFSETS, SLOTS, half), bf16),
                dma((4,)), dma((3,)), dma((3,)), dma((4,)), dma((4,)), dma((5,)),
                rounds, rounds, rounds, rounds, rounds,
            ],
            compiler_params=pltpu.CompilerParams(collective_id=0, has_side_effects=True),
            name="experts",
        )(tokens, norm_gain.reshape(1, half), routing.T, route_weight.T, w_gate, w_up, w_down)

    in_specs = (
        P("ep", "tp"), P("tp"), P("ep", None), P("ep", None),
        P("ep", None, "tp"), P("ep", None, "tp"), P("ep", None, "tp"),
    )
    return jax.shard_map(local, mesh=mesh, in_specs=in_specs, out_specs=P("ep", "tp"), check_vma=False)
```

```python
import functools

import jax
import jax.numpy as jnp
from jax import lax
from jax.experimental import pallas as pl
from jax.experimental.pallas import tpu as pltpu
from jax.sharding import PartitionSpec as P

CAP = 8
EPSILON = 1e-06
MESH = pl.DeviceIdType.MESH

Z, Y, X = 8, 4, 4
EXPERTS = 2 * X
SLOTS = EXPERTS * CAP // 2
OFFSETS = Z * Y
STEPS = (0, 1, 7, 2, 6, 3, 5, 4)
ROUNDS = tuple((p, p + 1) for p in range(Z))
SEND_ORDER = (0, 1, 4, 6, 5, 3, 2, 7)
ORDER = (
    "A0", "A1", "A4", "F1", "F4", "A5", "A6", "F5", "C4", "A7", "C1", "F6", "A3", "C5", "F7", "A2",
    "C6", "F3", "C7", "F2", "F0", "C3", "C2", "C0", "H4", "H1", "H5", "H6", "H7", "H3", "H2", "H0",
)


def kernel(
    tok_hbm, gain_hbm, routing_hbm, weight_hbm, wg_hbm, wu_hbm, wd_hbm, out_ref,
    tok, routing, weight, gains, wg, wu, wd, give_g, give_u, give_d,
    meta_s, meta_r, pick_home, send_1, recv_1, send_2, recv_2, send_3, recv_3, send_4, recv_4,
    in_sem, own_sem, give_sem, far_send, far_recv, s_sem, meta_sem, sem_1, sem_2, sem_3, sem_4,
):
    me, core = lax.axis_index("ep"), lax.axis_index("tp")
    other = 1 - core
    z, y, x = me // (Y * X), me // X % Y, me % X
    tokens, half = tok.shape

    def plane(step, dy, sign):
        if sign > 0:
            return ((z + step) % Z * Y + (y + dy) % Y) * X + x
        return ((z + Z - step) % Z * Y + (y + Y - dy) % Y) * X + x

    def line(dx, sign):
        return me - x + (x + (dx if sign > 0 else X - dx)) % X

    stores = ((wg_hbm, wg, give_g), (wu_hbm, wu, give_u), (wd_hbm, wd, give_d))
    inputs = ((routing_hbm, routing), (weight_hbm, weight), (tok_hbm, tok), (gain_hbm, gains.at[core]))
    inputs = [pltpu.make_async_copy(src, dst, in_sem.at[i]) for i, (src, dst) in enumerate(inputs)]
    own = [
        pltpu.make_async_copy(src.at[core], dst.at[core], own_sem.at[i])
        for i, (src, dst, _) in enumerate(stores)
    ]
    give = [
        pltpu.make_async_copy(src.at[other], stage, give_sem.at[i])
        for i, (src, _, stage) in enumerate(stores)
    ]
    for copy in inputs:
        copy.start()

    barrier = pltpu.get_barrier_semaphore()
    greeted = 0
    for step in STEPS:
        for dy in range(Y):
            if step or dy:
                pl.semaphore_signal(barrier, inc=1, device_id=(plane(step, dy, 1), core), device_id_type=MESH)
                greeted += 1
    for dx in range(X):
        for c in range(2):
            if dx:
                pl.semaphore_signal(barrier, inc=1, device_id=(line(dx, 1), c), device_id_type=MESH)
                greeted += 1
    pl.semaphore_signal(barrier, inc=1, device_id=(me, other), device_id_type=MESH)
    greeted += 1
    for copy in give + own:
        copy.start()

    row = lax.broadcasted_iota(jnp.int32, (tokens, tokens), 0)
    col = lax.broadcasted_iota(jnp.int32, (tokens, tokens), 1)
    before = (row < col).astype(jnp.float32).astype(jnp.bfloat16)
    names = lax.broadcasted_iota(jnp.int32, (OFFSETS * EXPERTS, tokens), 0)
    inputs[0].wait()
    picks = [routing[k:k + 1, :] for k in range(2)]
    group = picks[0] // EXPERTS
    dz = (group // Y - z + Z) % Z
    dy = (group % Y - y + Y) % Y
    place = jnp.where(dz <= Z // 2, jnp.maximum(2 * dz - 1, 0), 2 * (Z - dz)) * Y + dy
    hot = [(picks[k] == names).astype(jnp.float32) for k in range(2)]
    hot_place = (place == names[:OFFSETS]).astype(jnp.float32)
    both = jnp.concatenate([hot[0] + hot[1], hot_place], axis=0).astype(jnp.bfloat16)
    earlier = jnp.dot(both, before, preferred_element_type=jnp.float32)
    slot = jnp.sum(earlier[OFFSETS * EXPERTS:] * hot_place, axis=0, keepdims=True)
    spot = place.astype(jnp.float32) * SLOTS + slot
    codes = [
        (picks[k] % EXPERTS * CAP + 1).astype(jnp.float32)
        + jnp.sum(earlier[:OFFSETS * EXPERTS] * hot[k], axis=0, keepdims=True)
        for k in range(2)
    ]
    inputs[1].wait()
    rows = [spot] + codes + [weight[k:k + 1, :] for k in range(2)] + [jnp.zeros_like(spot)] * 3
    columns = jnp.transpose(jnp.concatenate(rows, axis=0))
    slots = OFFSETS * SLOTS
    lanes = lax.broadcasted_iota(jnp.int32, (tokens, slots), 1)
    at_home = lanes == columns[:, 0:1].astype(jnp.int32)
    pick_home[...] = at_home.astype(jnp.float32).astype(jnp.bfloat16)
    for q in range(4):
        values = jnp.sum(jnp.where(at_home, columns[:, q + 1:q + 2], 0.0), axis=0, keepdims=True)
        for p in range(Z):
            meta_s[p, q:q + 1, :] = values[:, p * Y * SLOTS:(p + 1) * Y * SLOTS]
    spread = lax.broadcasted_iota(jnp.int32, (slots, tokens), 0) == spot.astype(jnp.int32)
    spread = spread.astype(jnp.float32).astype(jnp.bfloat16)
    inputs[2].wait()
    outgoing = jnp.dot(spread, tok[...], preferred_element_type=jnp.float32)
    send_1[...] = outgoing.astype(jnp.bfloat16).reshape(OFFSETS, SLOTS, half)
    inputs[3].wait()

    pl.semaphore_wait(barrier, greeted)

    def remote(src, dst, send, recv, peer, c):
        return pltpu.make_async_remote_copy(
            src_ref=src, dst_ref=dst, send_sem=send, recv_sem=recv,
            device_id=(peer, c), device_id_type=MESH,
        )

    pltpu.make_async_copy(meta_s.at[0], meta_r.at[0], meta_sem.at[0]).start()
    pltpu.make_async_copy(send_1.at[0], recv_1.at[0], sem_1.at[0]).start()
    for r in SEND_ORDER:
        for dy in range(Y):
            for p in range(*ROUNDS[r]):
                if p or dy:
                    o, peer = p * Y + dy, plane(STEPS[p], dy, 1)
                    remote(meta_s.at[p], meta_r.at[o], s_sem.at[0], meta_sem.at[r], peer, core).start()
                    remote(send_1.at[o], recv_1.at[o], s_sem.at[1], sem_1.at[r], peer, core).start()

    gain_copy = remote(gains.at[core], gains.at[core], far_send.at[3], far_recv.at[3], me, other)
    gain_copy.start()
    for copy in give:
        copy.wait()
    far = [
        remote(stage, dst.at[core], far_send.at[i], far_recv.at[i], me, other)
        for i, (_, dst, stage) in enumerate(stores)
    ]
    for copy in far:
        copy.start()

    def arrived(ref, sem):
        pltpu.make_async_copy(ref, ref, sem).wait()

    def codes_of(r):
        parts = []
        segment = lax.broadcasted_iota(jnp.int32, (4, Y * SLOTS), 1) // SLOTS
        for p in range(*ROUNDS[r]):
            part = jnp.zeros((4, Y * SLOTS), jnp.float32)
            for dy in range(Y):
                part = jnp.where(segment == dy, meta_r[p * Y + dy], part)
            parts.append(part)
        return parts

    def full(code, block, blocks):
        code = code.astype(jnp.int32) - 1
        return (code >> 3) * (blocks * CAP) + block * CAP + (code & 7)

    def extent(r):
        first, last = ROUNDS[r]
        return first * Y, (last - first) * Y

    def step_a(r):
        first, blocks = extent(r)
        here = pl.ds(first, blocks)
        arrived(meta_r.at[here], meta_sem.at[r])
        table = codes_of(r)
        table = jnp.concatenate(table, axis=1) if len(table) > 1 else table[0]
        block = lax.broadcasted_iota(jnp.int32, (1, blocks * SLOTS), 1) // SLOTS
        places = lax.broadcasted_iota(jnp.int32, (EXPERTS * blocks * CAP, blocks * SLOTS), 0)
        hit = [places == full(table[k:k + 1, :], block, blocks) for k in range(2)]
        pick = (hit[0] | hit[1]).astype(jnp.float32).astype(jnp.bfloat16)
        arrived(recv_1.at[here], sem_1.at[r])
        source = recv_1[first:first + blocks].reshape(blocks * SLOTS, half)
        lined = jnp.dot(pick, source, preferred_element_type=jnp.float32).astype(jnp.bfloat16)
        at = pl.ds(first * CAP, blocks * CAP)
        send_2[:, first * CAP:(first + blocks) * CAP, :] = lined.reshape(EXPERTS, blocks * CAP, half)
        for dx in (2, 1, 3):
            peer = line(dx, 1)
            for c in range(2):
                remote(
                    send_2.at[(x + dx) % X * 2 + c, at], recv_2.at[dx, core, at], s_sem.at[2], sem_2.at[r], peer, c
                ).start()
        remote(send_2.at[x * 2 + other, at], recv_2.at[0, core, at], s_sem.at[2], sem_2.at[r], me, other).start()
        pltpu.make_async_copy(send_2.at[x * 2 + core, at], recv_2.at[0, core, at], sem_2.at[r]).start()

    ready = []

    def step_f(r):
        first, blocks = extent(r)
        count = blocks * CAP
        at = pl.ds(first * CAP, count)
        arrived(recv_2.at[:, :, at], sem_2.at[r])
        if not ready:
            gain_copy.wait()
        parts = [
            recv_2[:, h, first * CAP:first * CAP + count, :].astype(jnp.float32).reshape(X * count, half)
            for h in range(2)
        ]
        squares = sum(jnp.sum(p * p, axis=1, keepdims=True) for p in parts)
        scale = lax.rsqrt(squares / (2 * half) + EPSILON)
        normed = jnp.concatenate(
            [(p * scale * gains[h]).astype(jnp.bfloat16) for h, p in enumerate(parts)], axis=1
        )
        if not ready:
            for copy in own + far[:2]:
                copy.wait()
        hidden = []
        for h in range(2):
            gate = jnp.dot(normed, wg[h], preferred_element_type=jnp.float32)
            up = jnp.dot(normed, wu[h], preferred_element_type=jnp.float32)
            hidden.append((jax.nn.silu(gate) * up).astype(jnp.bfloat16))
        hidden = jnp.concatenate(hidden, axis=1)
        if not ready:
            far[2].wait()
            ready.append(True)
        for f in range(2):
            result = jnp.dot(hidden, wd[f], preferred_element_type=jnp.float32).astype(jnp.bfloat16)
            send_3[:, f, first * CAP:first * CAP + count, :] = result.reshape(X, count, half)
        mine = x * 2 + core
        for dx in (2, 1, 3):
            peer = line(dx, -1)
            for c in range(2):
                remote(
                    send_3.at[dx, c, at], recv_3.at[mine, at], s_sem.at[3], sem_3.at[r], peer, c
                ).start()
        remote(send_3.at[0, other, at], recv_3.at[mine, at], s_sem.at[3], sem_3.at[r], me, other).start()
        pltpu.make_async_copy(send_3.at[0, core, at], recv_3.at[mine, at], sem_3.at[r]).start()

    def step_c(r):
        first, blocks = extent(r)
        at = pl.ds(first * CAP, blocks * CAP)
        table = [jnp.transpose(jnp.concatenate([t, jnp.zeros_like(t)], axis=0)) for t in codes_of(r)]
        table = jnp.concatenate(table, axis=0) if len(table) > 1 else table[0]
        block = lax.broadcasted_iota(jnp.int32, (blocks * SLOTS, 1), 0) // SLOTS
        places = lax.broadcasted_iota(jnp.int32, (blocks * SLOTS, EXPERTS * blocks * CAP), 1)
        take = [
            (places == full(table[:, k:k + 1], block, blocks)).astype(jnp.float32).astype(jnp.bfloat16)
            for k in range(2)
        ]
        arrived(recv_3.at[:, at], sem_3.at[r])
        source = recv_3[:, first * CAP:(first + blocks) * CAP, :].reshape(EXPERTS * blocks * CAP, half)
        total = 0.0
        for k in range(2):
            total = total + table[:, 2 + k:3 + k] * jnp.dot(take[k], source, preferred_element_type=jnp.float32)
        send_4[first:first + blocks] = total.astype(jnp.bfloat16).reshape(blocks, SLOTS, half)
        for dy in range(Y):
            for p in range(*ROUNDS[r]):
                o = p * Y + dy
                if o:
                    remote(
                        send_4.at[o], recv_4.at[o], s_sem.at[4], sem_4.at[r], plane(STEPS[p], dy, -1), core
                    ).start()
                else:
                    pltpu.make_async_copy(send_4.at[0], recv_4.at[0], sem_4.at[r]).start()

    sums = []

    def step_h(r):
        first, blocks = extent(r)
        here = pl.ds(first, blocks)
        arrived(recv_4.at[here], sem_4.at[r])
        source = recv_4[first:first + blocks].reshape(blocks * SLOTS, half)
        take = pick_home[:, first * SLOTS:(first + blocks) * SLOTS]
        sums.append(jnp.dot(take, source, preferred_element_type=jnp.float32))

    step_of = {"A": step_a, "F": step_f, "C": step_c, "H": step_h}
    for name in ORDER:
        step_of[name[0]](int(name[1]))
    out_ref[...] = sum(sums).astype(jnp.bfloat16)

    arrived(meta_r.at[pl.ds(1, OFFSETS - 1)], s_sem.at[0])
    arrived(send_1.at[pl.ds(1, OFFSETS - 1)], s_sem.at[1])
    arrived(send_2.at[pl.ds(1, EXPERTS - 1)], s_sem.at[2])
    arrived(send_2.at[pl.ds(1, EXPERTS - 1)], s_sem.at[3])
    arrived(send_4.at[pl.ds(1, OFFSETS - 1)], s_sem.at[4])


def solution(mesh):
    assert mesh.shape["ep"] == Z * Y * X and mesh.shape["tp"] == 2

    def local(tokens, norm_gain, routing, route_weight, w_gate, w_up, w_down):
        rows, half = tokens.shape
        vmem = pl.BlockSpec(memory_space=pltpu.VMEM)
        far = pl.BlockSpec(memory_space=pl.ANY)
        dma = pltpu.SemaphoreType.DMA
        bf16, f32 = jnp.bfloat16, jnp.float32
        blocks = OFFSETS * CAP
        rounds = dma((len(ROUNDS),))
        return pl.pallas_call(
            kernel,
            out_shape=pltpu.VMEM((rows, half), bf16),
            in_specs=[far] * 7,
            out_specs=vmem,
            scratch_shapes=[
                pltpu.VMEM((rows, half), bf16),
                pltpu.VMEM((2, rows), jnp.int32),
                pltpu.VMEM((2, rows), f32),
                pltpu.VMEM((2, 1, half), f32),
                pltpu.VMEM(w_gate.shape, bf16),
                pltpu.VMEM(w_up.shape, bf16),
                pltpu.VMEM(w_down.shape, bf16),
                pltpu.VMEM(w_gate.shape[1:], bf16),
                pltpu.VMEM(w_up.shape[1:], bf16),
                pltpu.VMEM(w_down.shape[1:], bf16),
                pltpu.VMEM((Z, 4, Y * SLOTS), f32),
                pltpu.VMEM((OFFSETS, 4, Y * SLOTS), f32),
                pltpu.VMEM((rows, OFFSETS * SLOTS), bf16),
                pltpu.VMEM((OFFSETS, SLOTS, half), bf16),
                pltpu.VMEM((OFFSETS, SLOTS, half), bf16),
                pltpu.VMEM((EXPERTS, blocks, half), bf16),
                pltpu.VMEM((X, 2, blocks, half), bf16),
                pltpu.VMEM((X, 2, blocks, half), bf16),
                pltpu.VMEM((EXPERTS, blocks, half), bf16),
                pltpu.VMEM((OFFSETS, SLOTS, half), bf16),
                pltpu.VMEM((OFFSETS, SLOTS, half), bf16),
                dma((4,)), dma((3,)), dma((3,)), dma((4,)), dma((4,)), dma((5,)),
                rounds, rounds, rounds, rounds, rounds,
            ],
            compiler_params=pltpu.CompilerParams(collective_id=0, has_side_effects=True),
            name="experts",
        )(tokens, norm_gain.reshape(1, half), routing.T, route_weight.T, w_gate, w_up, w_down)

    in_specs = (
        P("ep", "tp"), P("tp"), P("ep", None), P("ep", None),
        P("ep", None, "tp"), P("ep", None, "tp"), P("ep", None, "tp"),
    )
    return jax.shard_map(local, mesh=mesh, in_specs=in_specs, out_specs=P("ep", "tp"), check_vma=False)
```

```python
import functools

import jax
import jax.numpy as jnp
from jax import lax
from jax.experimental import pallas as pl
from jax.experimental.pallas import tpu as pltpu
from jax.sharding import PartitionSpec as P

CAP = 8
EPSILON = 1e-06
MESH = pl.DeviceIdType.MESH

Z, Y, X = 8, 4, 4
EXPERTS = 2 * X
SLOTS = EXPERTS * CAP // 2
OFFSETS = Z * Y
STEPS = (0, 1, 7, 2, 6, 3, 5, 4)
LINE = (2, 1, 3)
COLUMN = (2, 1, 3)
ORDER = """
    G00 G01 G03 G02 A0 G10 G11 G13 G12 A1 A2 G20 G21 F0 G23 G22 A3 A4 F1 G30 G31 C0 G33 G32 A5 A6 F2 F3 C1
    A7 F4 C2 E0 F5 E1 C3 F6 E2 C4 F7 C5 E3 C6 E4 C7 E5 E6 E7 H0 H1 H2 H3 H4 H5 H6 H7
"""


def kernel(
    tok_hbm, gain_hbm, routing_hbm, weight_hbm, wg_hbm, wu_hbm, wd_hbm, out_ref,
    routing, weight, gains, wg, wu, wd, give_g, give_u, give_d,
    meta_s, meta_r, blocks, tables, send_2, recv_2, send_3, recv_3, send_4, recv_4, send_5, recv_5,
    in_sem, own_sem, give_sem, far_send, far_recv, s_sem, meta_sem, block_sem, table_sem, sem_2, sem_3, sem_4, sem_5,
):
    me, core = lax.axis_index("ep"), lax.axis_index("tp")
    other = 1 - core
    z, y, x = me // (Y * X), me // X % Y, me % X
    tokens, half = blocks.shape[2:]
    place_of = {step: p for p, step in enumerate(STEPS)}

    def plane(step, dy, sign):
        if sign > 0:
            return ((z + step) % Z * Y + (y + dy) % Y) * X + x
        return ((z + Z - step) % Z * Y + (y + Y - dy) % Y) * X + x

    def line(dx, sign):
        return me - x + (x + (dx if sign > 0 else X - dx)) % X

    stores = ((wg_hbm, wg, give_g), (wu_hbm, wu, give_u), (wd_hbm, wd, give_d))
    inputs = ((routing_hbm, routing), (weight_hbm, weight), (tok_hbm, blocks.at[0, 0]), (gain_hbm, gains.at[core]))
    inputs = [pltpu.make_async_copy(src, dst, in_sem.at[i]) for i, (src, dst) in enumerate(inputs)]
    own = [
        pltpu.make_async_copy(src.at[core], dst.at[core], own_sem.at[i])
        for i, (src, dst, _) in enumerate(stores)
    ]
    give = [
        pltpu.make_async_copy(src.at[other], stage, give_sem.at[i])
        for i, (src, _, stage) in enumerate(stores)
    ]
    for copy in inputs:
        copy.start()

    barrier = pltpu.get_barrier_semaphore()
    greeted = 0
    for step in STEPS:
        for dy in range(Y):
            if step or dy:
                pl.semaphore_signal(barrier, inc=1, device_id=(plane(step, dy, 1), core), device_id_type=MESH)
                greeted += 1
    for dy in range(1, Y):
        pl.semaphore_signal(barrier, inc=1, device_id=(plane(0, dy, 1), other), device_id_type=MESH)
        greeted += 1
    for dx in range(X):
        for c in range(2):
            if dx:
                pl.semaphore_signal(barrier, inc=1, device_id=(line(dx, 1), c), device_id_type=MESH)
                greeted += 1
    pl.semaphore_signal(barrier, inc=1, device_id=(me, other), device_id_type=MESH)
    greeted += 1
    for copy in give + own:
        copy.start()

    row = lax.broadcasted_iota(jnp.int32, (tokens, tokens), 0)
    col = lax.broadcasted_iota(jnp.int32, (tokens, tokens), 1)
    before = (row < col).astype(jnp.float32).astype(jnp.bfloat16)
    names = lax.broadcasted_iota(jnp.int32, (OFFSETS * EXPERTS, tokens), 0)
    inputs[0].wait()
    picks = [routing[k:k + 1, :] for k in range(2)]
    group = picks[0] // EXPERTS
    dz = (group // Y - z + Z) % Z
    dy = (group % Y - y + Y) % Y
    place = jnp.where(dz <= Z // 2, jnp.maximum(2 * dz - 1, 0), 2 * (Z - dz)) * Y + dy
    hot = [(picks[k] == names).astype(jnp.float32) for k in range(2)]
    hot_place = (place == names[:OFFSETS]).astype(jnp.float32)
    both = jnp.concatenate([hot[0] + hot[1], hot_place], axis=0).astype(jnp.bfloat16)
    earlier = jnp.dot(both, before, preferred_element_type=jnp.float32)
    slot = jnp.sum(earlier[OFFSETS * EXPERTS:] * hot_place, axis=0, keepdims=True)
    spot = place.astype(jnp.float32) * SLOTS + slot
    ranks = [jnp.sum(earlier[:OFFSETS * EXPERTS] * hot[k], axis=0, keepdims=True) for k in range(2)]
    codes = [(picks[k] % EXPERTS * CAP + 1).astype(jnp.float32) + ranks[k] for k in range(2)]
    seats = [(picks[k] * CAP).astype(jnp.float32) + ranks[k] for k in range(2)]
    inputs[1].wait()
    rows = [spot] + codes + [weight[k:k + 1, :] for k in range(2)] + seats + [spot]
    columns = jnp.transpose(jnp.concatenate(rows, axis=0))
    slots = OFFSETS * SLOTS
    lanes = lax.broadcasted_iota(jnp.int32, (tokens, slots), 1)
    at_home = lanes == columns[:, 0:1].astype(jnp.int32)
    for q in range(4):
        values = jnp.sum(jnp.where(at_home, columns[:, q + 1:q + 2], 0.0), axis=0, keepdims=True)
        for p in range(Z):
            meta_s[p, q:q + 1, :] = values[:, p * Y * SLOTS:(p + 1) * Y * SLOTS]
    repeated = lax.broadcasted_iota(jnp.int32, (tokens, X * tokens), 1) % tokens
    repeated = repeated == lax.broadcasted_iota(jnp.int32, (tokens, X * tokens), 0)
    for k in range(3):
        values = jnp.where(repeated, columns[:, 5 + k:6 + k], 0.0)
        tables[0, 0, k:k + 1, :] = jnp.sum(values, axis=0, keepdims=True)
    tables[0, 0, 3:4, :] = jnp.zeros((1, X * tokens), jnp.float32)
    inputs[2].wait()
    inputs[3].wait()

    pl.semaphore_wait(barrier, greeted)

    def remote(src, dst, send, recv, peer, c):
        return pltpu.make_async_remote_copy(
            src_ref=src, dst_ref=dst, send_sem=send, recv_sem=recv,
            device_id=(peer, c), device_id_type=MESH,
        )

    def arrived(ref, sem):
        pltpu.make_async_copy(ref, ref, sem).wait()

    def pass_on(p, j, q, i, peer):
        remote(tables.at[p, j], tables.at[q, i], s_sem.at[0], table_sem.at[q, i], peer, core).start()
        remote(blocks.at[p, j], blocks.at[q, i], s_sem.at[1], block_sem.at[q, i], peer, core).start()

    up, down = plane(1, 0, 1), plane(1, 0, -1)
    middle = Z // 2

    def step_g(k, j):
        for p in sorted({place_of[k], place_of[(Z - k) % Z]}):
            chunk_here(p, j)
        if k + 1 < middle or j < X // 2:
            pass_on(place_of[k], j, place_of[k + 1], j, up)
        if k + 1 < middle or j >= X // 2:
            pass_on(place_of[(Z - k) % Z], j, place_of[Z - k - 1], j, down)

    seen = {(0, 0)}

    def chunk_here(p, j):
        if (p, j) not in seen:
            seen.add((p, j))
            arrived(tables.at[p, j], table_sem.at[p, j])
            arrived(blocks.at[p, j], block_sem.at[p, j])

    for dx in LINE:
        pass_on(0, 0, 0, dx, line(dx, 1))
    step_g(0, 0)
    pltpu.make_async_copy(meta_s.at[0], meta_r.at[0], meta_sem.at[0]).start()
    for p, step in enumerate(STEPS):
        for dy in range(Y):
            if p or dy:
                o, peer = p * Y + dy, plane(step, dy, 1)
                remote(meta_s.at[p], meta_r.at[o], s_sem.at[2], meta_sem.at[p], peer, core).start()

    gain_copy = remote(gains.at[core], gains.at[core], far_send.at[3], far_recv.at[3], me, other)
    gain_copy.start()
    for copy in give:
        copy.wait()
    far = [
        remote(stage, dst.at[core], far_send.at[i], far_recv.at[i], me, other)
        for i, (_, dst, stage) in enumerate(stores)
    ]
    for copy in far:
        copy.start()

    def codes_of(p):
        segment = lax.broadcasted_iota(jnp.int32, (4, Y * SLOTS), 1) // SLOTS
        table = jnp.zeros((4, Y * SLOTS), jnp.float32)
        for dy in range(Y):
            table = jnp.where(segment == dy, meta_r[p * Y + dy], table)
        return table

    def step_a(p):
        for j in range(X):
            chunk_here(p, j)
        spot_of = lax.broadcasted_iota(jnp.int32, (4, X * tokens), 1) // tokens
        seat = jnp.zeros((4, X * tokens), jnp.float32)
        for j in range(X):
            seat = jnp.where(spot_of == j, tables[p, j], seat)
        seat = seat.astype(jnp.int32)
        pick = seat // CAP
        group, expert = pick // EXPERTS, pick % EXPERTS
        dy = (group % Y - y + Y) % Y
        target = ((dy * 2 + expert % 2) * X + spot_of) * CAP + seat % CAP
        target = jnp.where((group // Y == z) & (expert // 2 == x), target, -1)
        places = lax.broadcasted_iota(jnp.int32, (Y * 2 * X * CAP, X * tokens), 0)
        take = (places == target[0:1]) | (places == target[1:2])
        take = take.astype(jnp.float32).astype(jnp.bfloat16)
        source = blocks[p].reshape(X * tokens, half)
        chosen = jnp.dot(take, source, preferred_element_type=jnp.float32)
        send_2[p] = chosen.reshape(Y, 2, X, CAP, half).astype(jnp.bfloat16)
        for dy in COLUMN:
            for c in range(2):
                remote(
                    send_2.at[p, dy, c], recv_2.at[core, p, :, dy], s_sem.at[3], sem_2.at[p], plane(0, dy, 1), c
                ).start()
        remote(send_2.at[p, 0, other], recv_2.at[core, p, :, 0], s_sem.at[3], sem_2.at[p], me, other).start()
        pltpu.make_async_copy(send_2.at[p, 0, core], recv_2.at[core, p, :, 0], sem_2.at[p]).start()

    ready = []

    def step_f(p):
        count = Y * CAP
        at = pl.ds(p * count, count)
        arrived(recv_2.at[:, p], sem_2.at[p])
        if not ready:
            gain_copy.wait()
        parts = [recv_2[h, p].astype(jnp.float32).reshape(X * count, half) for h in range(2)]
        squares = sum(jnp.sum(part * part, axis=1, keepdims=True) for part in parts)
        scale = lax.rsqrt(squares / (2 * half) + EPSILON)
        normed = jnp.concatenate(
            [(part * scale * gains[h]).astype(jnp.bfloat16) for h, part in enumerate(parts)], axis=1
        )
        if not ready:
            for copy in own + far[:2]:
                copy.wait()
        hidden = []
        for h in range(2):
            gate = jnp.dot(normed, wg[h], preferred_element_type=jnp.float32)
            up = jnp.dot(normed, wu[h], preferred_element_type=jnp.float32)
            hidden.append((jax.nn.silu(gate) * up).astype(jnp.bfloat16))
        hidden = jnp.concatenate(hidden, axis=1)
        if not ready:
            far[2].wait()
            ready.append(True)
        for f in range(2):
            result = jnp.dot(hidden, wd[f], preferred_element_type=jnp.float32).astype(jnp.bfloat16)
            send_3[:, f, p * count:(p + 1) * count, :] = result.reshape(X, count, half)
        mine = x * 2 + core
        for dx in LINE:
            peer = line(dx, -1)
            for c in range(2):
                remote(
                    send_3.at[dx, c, at], recv_3.at[mine, at], s_sem.at[4], sem_3.at[p], peer, c
                ).start()
        remote(send_3.at[0, other, at], recv_3.at[mine, at], s_sem.at[4], sem_3.at[p], me, other).start()
        pltpu.make_async_copy(send_3.at[0, core, at], recv_3.at[mine, at], sem_3.at[p]).start()

    def step_c(p):
        arrived(meta_r.at[pl.ds(p * Y, Y)], meta_sem.at[p])
        table = codes_of(p)
        table = jnp.transpose(jnp.concatenate([table, jnp.zeros_like(table)], axis=0))
        block = lax.broadcasted_iota(jnp.int32, (Y * SLOTS, 1), 0) // SLOTS
        places = lax.broadcasted_iota(jnp.int32, (Y * SLOTS, EXPERTS * Y * CAP), 1)
        take = []
        for k in range(2):
            code = table[:, k:k + 1].astype(jnp.int32) - 1
            code = (code >> 3) * (Y * CAP) + block * CAP + (code & 7)
            take.append((places == code).astype(jnp.float32).astype(jnp.bfloat16))
        at = pl.ds(p * Y * CAP, Y * CAP)
        arrived(recv_3.at[:, at], sem_3.at[p])
        source = recv_3[:, p * Y * CAP:(p + 1) * Y * CAP, :].reshape(EXPERTS * Y * CAP, half)
        total = 0.0
        for k in range(2):
            total = total + table[:, 2 + k:3 + k] * jnp.dot(take[k], source, preferred_element_type=jnp.float32)
        send_4[p * Y:(p + 1) * Y] = total.astype(jnp.bfloat16).reshape(Y, SLOTS, half)
        for dy in COLUMN:
            o = p * Y + dy
            remote(send_4.at[o], recv_4.at[o], s_sem.at[5], sem_4.at[p], plane(0, dy, -1), core).start()
        pltpu.make_async_copy(send_4.at[p * Y], recv_4.at[p * Y], sem_4.at[p]).start()

    def step_e(p):
        table = tables[p, 0, :, :2 * tokens]
        table = jnp.transpose(jnp.concatenate([table, jnp.zeros_like(table)], axis=0))
        spot = table[:tokens, 2:3].astype(jnp.int32) - p * Y * SLOTS
        places = lax.broadcasted_iota(jnp.int32, (tokens, Y * SLOTS), 1)
        take = (places == spot).astype(jnp.float32).astype(jnp.bfloat16)
        arrived(recv_4.at[pl.ds(p * Y, Y)], sem_4.at[p])
        source = recv_4[p * Y:(p + 1) * Y].reshape(Y * SLOTS, half)
        send_5[p] = jnp.dot(take, source, preferred_element_type=jnp.float32).astype(jnp.bfloat16)
        if p:
            remote(send_5.at[p], recv_5.at[p], s_sem.at[6], sem_5.at[p], plane(STEPS[p], 0, -1), core).start()
        else:
            pltpu.make_async_copy(send_5.at[0], recv_5.at[0], sem_5.at[0]).start()

    sums = []

    def step_h(p):
        arrived(recv_5.at[p], sem_5.at[p])
        sums.append(recv_5[p].astype(jnp.float32))

    step_of = {"G": step_g, "A": step_a, "F": step_f, "C": step_c, "E": step_e, "H": step_h}
    for name in ORDER.split():
        if name != "G00":
            step_of[name[0]](*map(int, name[1:]))
    out_ref[...] = sum(sums).astype(jnp.bfloat16)

    for at in ((pl.ds(1, Z - 1),), (0, pl.ds(1, X - 1))):
        arrived(tables.at[at], s_sem.at[0])
        arrived(blocks.at[at], s_sem.at[1])
    arrived(meta_r.at[pl.ds(1, OFFSETS - 1)], s_sem.at[2])
    arrived(recv_2.at[0, :, :, pl.ds(1, Y - 1)], s_sem.at[3])
    arrived(recv_2.at[1], s_sem.at[3])
    arrived(recv_3.at[pl.ds(1, EXPERTS - 1)], s_sem.at[4])
    arrived(send_4.at[pl.ds(0, OFFSETS - Z)], s_sem.at[5])
    arrived(send_5.at[pl.ds(1, Z - 1)], s_sem.at[6])


def solution(mesh):
    assert mesh.shape["ep"] == Z * Y * X and mesh.shape["tp"] == 2

    def local(tokens, norm_gain, routing, route_weight, w_gate, w_up, w_down):
        rows, half = tokens.shape
        vmem = pl.BlockSpec(memory_space=pltpu.VMEM)
        far = pl.BlockSpec(memory_space=pl.ANY)
        dma = pltpu.SemaphoreType.DMA
        bf16, f32 = jnp.bfloat16, jnp.float32
        line_rows = OFFSETS * CAP
        rounds = dma((Z,))
        return pl.pallas_call(
            kernel,
            out_shape=pltpu.VMEM((rows, half), bf16),
            in_specs=[far] * 7,
            out_specs=vmem,
            scratch_shapes=[
                pltpu.VMEM((2, rows), jnp.int32),
                pltpu.VMEM((2, rows), f32),
                pltpu.VMEM((2, 1, half), f32),
                pltpu.VMEM(w_gate.shape, bf16),
                pltpu.VMEM(w_up.shape, bf16),
                pltpu.VMEM(w_down.shape, bf16),
                pltpu.VMEM(w_gate.shape[1:], bf16),
                pltpu.VMEM(w_up.shape[1:], bf16),
                pltpu.VMEM(w_down.shape[1:], bf16),
                pltpu.VMEM((Z, 4, Y * SLOTS), f32),
                pltpu.VMEM((OFFSETS, 4, Y * SLOTS), f32),
                pltpu.VMEM((Z, X, rows, half), bf16),
                pltpu.VMEM((Z, X, 4, X * rows), f32),
                pltpu.VMEM((Z, Y, 2, X, CAP, half), bf16),
                pltpu.VMEM((2, Z, X, Y, CAP, half), bf16),
                pltpu.VMEM((X, 2, line_rows, half), bf16),
                pltpu.VMEM((EXPERTS, line_rows, half), bf16),
                pltpu.VMEM((OFFSETS, SLOTS, half), bf16),
                pltpu.VMEM((OFFSETS, SLOTS, half), bf16),
                pltpu.VMEM((Z, rows, half), bf16),
                pltpu.VMEM((Z, rows, half), bf16),
                dma((4,)), dma((3,)), dma((3,)), dma((4,)), dma((4,)), dma((7,)),
                rounds, dma((Z, X)), dma((Z, X)), rounds, rounds, rounds, rounds,
            ],
            compiler_params=pltpu.CompilerParams(collective_id=0, has_side_effects=True),
            name="experts",
        )(tokens, norm_gain.reshape(1, half), routing.T, route_weight.T, w_gate, w_up, w_down)

    in_specs = (
        P("ep", "tp"), P("tp"), P("ep", None), P("ep", None),
        P("ep", None, "tp"), P("ep", None, "tp"), P("ep", None, "tp"),
    )
    return jax.shard_map(local, mesh=mesh, in_specs=in_specs, out_specs=P("ep", "tp"), check_vma=False)
```

```python
import functools

import jax
import jax.numpy as jnp
from jax import lax
from jax.experimental import pallas as pl
from jax.experimental.pallas import tpu as pltpu
from jax.sharding import PartitionSpec as P

CAP = 8
EPSILON = 1e-06
MESH = pl.DeviceIdType.MESH

Z, Y, X = 8, 4, 4
EXPERTS = 2 * X
SLOTS = EXPERTS * CAP // 2
OFFSETS = Z * Y
STEPS = (0, 1, 7, 2, 6, 3, 5, 4)
LINE = (2, 1, 3)
GATHER = (1, 3, 2)
COLUMN = (2, 1, 3)
ORDER = """
    G00 G01 A00 G02 G03 G10 A01 A10 A20 G11 G12 A21 G13 A11 F0 A40 G21 A30 G20 A31 G23 F2 G22 A41 G30 A60 G31
    A50 F3 G33 A61 A51 G32 F4 A70 F6 A71 C3 F5 C4 F7 C6 F1 E4 C5 C2 E3 E6 C7 E5 C1 H3 E7 C0 E2 E1 E0 H4 H0 H6 H2
    H5 H1 H7
"""


def kernel(
    tok_hbm, gain_hbm, routing_hbm, weight_hbm, wg_hbm, wu_hbm, wd_hbm, out_ref,
    routing, weight, gains, wg, wu, wd, give_g, give_u, give_d,
    meta_s, meta_r, blocks, tables, send_2, recv_2, send_3, recv_3, send_4, recv_4, send_5, recv_5,
    in_sem, own_sem, give_sem, far_send, far_recv, s_sem, meta_sem, block_sem, table_sem, sem_2, sem_3, sem_4, sem_5,
):
    me, core = lax.axis_index("ep"), lax.axis_index("tp")
    other = 1 - core
    z, y, x = me // (Y * X), me // X % Y, me % X
    tokens, half = blocks.shape[2:]
    place_of = {step: p for p, step in enumerate(STEPS)}

    def plane(step, dy, sign):
        if sign > 0:
            return ((z + step) % Z * Y + (y + dy) % Y) * X + x
        return ((z + Z - step) % Z * Y + (y + Y - dy) % Y) * X + x

    def line(dx, sign):
        return me - x + (x + (dx if sign > 0 else X - dx)) % X

    stores = ((wg_hbm, wg, give_g), (wu_hbm, wu, give_u), (wd_hbm, wd, give_d))
    inputs = ((routing_hbm, routing), (weight_hbm, weight), (tok_hbm, blocks.at[0, 0]), (gain_hbm, gains.at[core]))
    inputs = [pltpu.make_async_copy(src, dst, in_sem.at[i]) for i, (src, dst) in enumerate(inputs)]
    own = [
        pltpu.make_async_copy(src.at[core], dst.at[core], own_sem.at[i])
        for i, (src, dst, _) in enumerate(stores)
    ]
    give = [
        pltpu.make_async_copy(src.at[other], stage, give_sem.at[i])
        for i, (src, _, stage) in enumerate(stores)
    ]
    for copy in inputs:
        copy.start()

    barrier = pltpu.get_barrier_semaphore()
    greeted = 0
    for step in STEPS:
        for dy in range(Y):
            if step or dy:
                pl.semaphore_signal(barrier, inc=1, device_id=(plane(step, dy, 1), core), device_id_type=MESH)
                greeted += 1
    for dy in range(1, Y):
        pl.semaphore_signal(barrier, inc=1, device_id=(plane(0, dy, 1), other), device_id_type=MESH)
        greeted += 1
    for dx in range(X):
        for c in range(2):
            if dx:
                pl.semaphore_signal(barrier, inc=1, device_id=(line(dx, 1), c), device_id_type=MESH)
                greeted += 1
    pl.semaphore_signal(barrier, inc=1, device_id=(me, other), device_id_type=MESH)
    greeted += 1
    for copy in give + own:
        copy.start()

    row = lax.broadcasted_iota(jnp.int32, (tokens, tokens), 0)
    col = lax.broadcasted_iota(jnp.int32, (tokens, tokens), 1)
    before = (row < col).astype(jnp.float32).astype(jnp.bfloat16)
    names = lax.broadcasted_iota(jnp.int32, (OFFSETS * EXPERTS, tokens), 0)
    inputs[0].wait()
    picks = [routing[k:k + 1, :] for k in range(2)]
    group = picks[0] // EXPERTS
    dz = (group // Y - z + Z) % Z
    dy = (group % Y - y + Y) % Y
    place = jnp.where(dz <= Z // 2, jnp.maximum(2 * dz - 1, 0), 2 * (Z - dz)) * Y + dy
    hot = [(picks[k] == names).astype(jnp.float32) for k in range(2)]
    hot_place = (place == names[:OFFSETS]).astype(jnp.float32)
    both = jnp.concatenate([hot[0] + hot[1], hot_place], axis=0).astype(jnp.bfloat16)
    earlier = jnp.dot(both, before, preferred_element_type=jnp.float32)
    slot = jnp.sum(earlier[OFFSETS * EXPERTS:] * hot_place, axis=0, keepdims=True)
    spot = place.astype(jnp.float32) * SLOTS + slot
    ranks = [jnp.sum(earlier[:OFFSETS * EXPERTS] * hot[k], axis=0, keepdims=True) for k in range(2)]
    codes = [(picks[k] % EXPERTS * CAP + 1).astype(jnp.float32) + ranks[k] for k in range(2)]
    seats = [(picks[k] * CAP).astype(jnp.float32) + ranks[k] for k in range(2)]
    inputs[1].wait()
    rows = [spot] + codes + [weight[k:k + 1, :] for k in range(2)] + seats + [spot]
    columns = jnp.transpose(jnp.concatenate(rows, axis=0))
    slots = OFFSETS * SLOTS
    lanes = lax.broadcasted_iota(jnp.int32, (tokens, slots), 1)
    at_home = lanes == columns[:, 0:1].astype(jnp.int32)
    for q in range(4):
        values = jnp.sum(jnp.where(at_home, columns[:, q + 1:q + 2], 0.0), axis=0, keepdims=True)
        for p in range(Z):
            meta_s[p, q:q + 1, :] = values[:, p * Y * SLOTS:(p + 1) * Y * SLOTS]
    repeated = lax.broadcasted_iota(jnp.int32, (tokens, 2 * tokens), 1) % tokens
    repeated = repeated == lax.broadcasted_iota(jnp.int32, (tokens, 2 * tokens), 0)
    for k in range(3):
        values = jnp.where(repeated, columns[:, 5 + k:6 + k], 0.0)
        tables[0, 0, k:k + 1, :] = jnp.sum(values, axis=0, keepdims=True)
    tables[0, 0, 3:4, :] = jnp.zeros((1, 2 * tokens), jnp.float32)
    inputs[2].wait()
    inputs[3].wait()

    pl.semaphore_wait(barrier, greeted)

    def remote(src, dst, send, recv, peer, c):
        return pltpu.make_async_remote_copy(
            src_ref=src, dst_ref=dst, send_sem=send, recv_sem=recv,
            device_id=(peer, c), device_id_type=MESH,
        )

    def arrived(ref, sem):
        pltpu.make_async_copy(ref, ref, sem).wait()

    def pass_on(p, j, q, i, peer):
        remote(tables.at[p, j], tables.at[q, i], s_sem.at[0], table_sem.at[q, i], peer, core).start()
        remote(blocks.at[p, j], blocks.at[q, i], s_sem.at[1], block_sem.at[q, i], peer, core).start()

    up, down = plane(1, 0, 1), plane(1, 0, -1)
    middle = Z // 2

    def step_g(k, j):
        for p in sorted({place_of[k], place_of[(Z - k) % Z]}):
            chunk_here(p, j)
        if k + 1 < middle or j < X // 2:
            pass_on(place_of[k], j, place_of[k + 1], j, up)
        if k + 1 < middle or j >= X // 2:
            pass_on(place_of[(Z - k) % Z], j, place_of[Z - k - 1], j, down)

    seen = {(0, 0)}

    def chunk_here(p, j):
        if (p, j) not in seen:
            seen.add((p, j))
            arrived(tables.at[p, j], table_sem.at[p, j])
            arrived(blocks.at[p, j], block_sem.at[p, j])

    for dx in GATHER:
        pass_on(0, 0, 0, dx, line(dx, 1))
    step_g(0, 0)
    pltpu.make_async_copy(meta_s.at[0], meta_r.at[0], meta_sem.at[0]).start()
    for p, step in enumerate(STEPS):
        for dy in range(Y):
            if p or dy:
                o, peer = p * Y + dy, plane(step, dy, 1)
                remote(meta_s.at[p], meta_r.at[o], s_sem.at[2], meta_sem.at[p], peer, core).start()

    gain_copy = remote(gains.at[core], gains.at[core], far_send.at[3], far_recv.at[3], me, other)
    gain_copy.start()
    for copy in give:
        copy.wait()
    far = [
        remote(stage, dst.at[core], far_send.at[i], far_recv.at[i], me, other)
        for i, (_, dst, stage) in enumerate(stores)
    ]
    for copy in far:
        copy.start()

    def codes_of(p):
        segment = lax.broadcasted_iota(jnp.int32, (4, Y * SLOTS), 1) // SLOTS
        table = jnp.zeros((4, Y * SLOTS), jnp.float32)
        for dy in range(Y):
            table = jnp.where(segment == dy, meta_r[p * Y + dy], table)
        return table

    def step_a(p, h):
        pair = X // 2
        for j in range(h * pair, h * pair + pair):
            chunk_here(p, j)
        at = pl.ds(h * pair, pair)
        spot_of = lax.broadcasted_iota(jnp.int32, (4, pair * tokens), 1) // tokens
        seat = jnp.zeros((4, pair * tokens), jnp.float32)
        for j in range(pair):
            seat = jnp.where(spot_of == j, tables[p, h * pair + j, :, :pair * tokens], seat)
        seat = seat.astype(jnp.int32)
        pick = seat // CAP
        group, expert = pick // EXPERTS, pick % EXPERTS
        dy = (group % Y - y + Y) % Y
        target = ((dy * 2 + expert % 2) * pair + spot_of) * CAP + seat % CAP
        target = jnp.where((group // Y == z) & (expert // 2 == x), target, -1)
        places = lax.broadcasted_iota(jnp.int32, (Y * 2 * pair * CAP, pair * tokens), 0)
        take = (places == target[0:1]) | (places == target[1:2])
        take = take.astype(jnp.float32).astype(jnp.bfloat16)
        source = blocks[p, h * pair:h * pair + pair].reshape(pair * tokens, half)
        chosen = jnp.dot(take, source, preferred_element_type=jnp.float32)
        send_2[p, h] = chosen.reshape(Y, 2, pair, CAP, half).astype(jnp.bfloat16)
        for dy in COLUMN:
            for c in range(2):
                remote(
                    send_2.at[p, h, dy, c], recv_2.at[core, p, at, dy], s_sem.at[3], sem_2.at[p], plane(0, dy, 1), c
                ).start()
        remote(send_2.at[p, h, 0, other], recv_2.at[core, p, at, 0], s_sem.at[3], sem_2.at[p], me, other).start()
        pltpu.make_async_copy(send_2.at[p, h, 0, core], recv_2.at[core, p, at, 0], sem_2.at[p]).start()

    ready = []

    def step_f(p):
        count = Y * CAP
        at = pl.ds(p * count, count)
        arrived(recv_2.at[:, p], sem_2.at[p])
        if not ready:
            gain_copy.wait()
        parts = [recv_2[h, p].astype(jnp.float32).reshape(X * count, half) for h in range(2)]
        squares = sum(jnp.sum(part * part, axis=1, keepdims=True) for part in parts)
        scale = lax.rsqrt(squares / (2 * half) + EPSILON)
        normed = jnp.concatenate(
            [(part * scale * gains[h]).astype(jnp.bfloat16) for h, part in enumerate(parts)], axis=1
        )
        if not ready:
            for copy in own + far[:2]:
                copy.wait()
        hidden = []
        for h in range(2):
            gate = jnp.dot(normed, wg[h], preferred_element_type=jnp.float32)
            up = jnp.dot(normed, wu[h], preferred_element_type=jnp.float32)
            hidden.append((jax.nn.silu(gate) * up).astype(jnp.bfloat16))
        hidden = jnp.concatenate(hidden, axis=1)
        if not ready:
            far[2].wait()
            ready.append(True)
        for f in range(2):
            result = jnp.dot(hidden, wd[f], preferred_element_type=jnp.float32).astype(jnp.bfloat16)
            send_3[:, f, p * count:(p + 1) * count, :] = result.reshape(X, count, half)
        mine = x * 2 + core
        for dx in LINE:
            peer = line(dx, -1)
            for c in range(2):
                remote(
                    send_3.at[dx, c, at], recv_3.at[mine, at], s_sem.at[4], sem_3.at[p], peer, c
                ).start()
        remote(send_3.at[0, other, at], recv_3.at[mine, at], s_sem.at[4], sem_3.at[p], me, other).start()
        pltpu.make_async_copy(send_3.at[0, core, at], recv_3.at[mine, at], sem_3.at[p]).start()

    def step_c(p):
        arrived(meta_r.at[pl.ds(p * Y, Y)], meta_sem.at[p])
        table = codes_of(p)
        table = jnp.transpose(jnp.concatenate([table, jnp.zeros_like(table)], axis=0))
        block = lax.broadcasted_iota(jnp.int32, (Y * SLOTS, 1), 0) // SLOTS
        places = lax.broadcasted_iota(jnp.int32, (Y * SLOTS, EXPERTS * Y * CAP), 1)
        take = []
        for k in range(2):
            code = table[:, k:k + 1].astype(jnp.int32) - 1
            code = (code >> 3) * (Y * CAP) + block * CAP + (code & 7)
            take.append((places == code).astype(jnp.float32).astype(jnp.bfloat16))
        at = pl.ds(p * Y * CAP, Y * CAP)
        arrived(recv_3.at[:, at], sem_3.at[p])
        source = recv_3[:, p * Y * CAP:(p + 1) * Y * CAP, :].reshape(EXPERTS * Y * CAP, half)
        total = 0.0
        for k in range(2):
            total = total + table[:, 2 + k:3 + k] * jnp.dot(take[k], source, preferred_element_type=jnp.float32)
        send_4[p * Y:(p + 1) * Y] = total.astype(jnp.bfloat16).reshape(Y, SLOTS, half)
        for dy in COLUMN:
            o = p * Y + dy
            remote(send_4.at[o], recv_4.at[o], s_sem.at[5], sem_4.at[p], plane(0, dy, -1), core).start()
        pltpu.make_async_copy(send_4.at[p * Y], recv_4.at[p * Y], sem_4.at[p]).start()

    def step_e(p):
        table = tables[p, 0]
        table = jnp.transpose(jnp.concatenate([table, jnp.zeros_like(table)], axis=0))
        spot = table[:tokens, 2:3].astype(jnp.int32) - p * Y * SLOTS
        places = lax.broadcasted_iota(jnp.int32, (tokens, Y * SLOTS), 1)
        take = (places == spot).astype(jnp.float32).astype(jnp.bfloat16)
        arrived(recv_4.at[pl.ds(p * Y, Y)], sem_4.at[p])
        source = recv_4[p * Y:(p + 1) * Y].reshape(Y * SLOTS, half)
        send_5[p] = jnp.dot(take, source, preferred_element_type=jnp.float32).astype(jnp.bfloat16)
        if p:
            remote(send_5.at[p], recv_5.at[p], s_sem.at[6], sem_5.at[p], plane(STEPS[p], 0, -1), core).start()
        else:
            pltpu.make_async_copy(send_5.at[0], recv_5.at[0], sem_5.at[0]).start()

    sums = []

    def step_h(p):
        arrived(recv_5.at[p], sem_5.at[p])
        sums.append(recv_5[p].astype(jnp.float32))

    step_of = {"G": step_g, "A": step_a, "F": step_f, "C": step_c, "E": step_e, "H": step_h}
    for name in ORDER.split():
        if name != "G00":
            step_of[name[0]](*map(int, name[1:]))
    out_ref[...] = sum(sums).astype(jnp.bfloat16)

    for at in ((pl.ds(1, Z - 1),), (0, pl.ds(1, X - 1))):
        arrived(tables.at[at], s_sem.at[0])
        arrived(blocks.at[at], s_sem.at[1])
    arrived(meta_r.at[pl.ds(1, OFFSETS - 1)], s_sem.at[2])
    arrived(recv_2.at[0, :, :, pl.ds(1, Y - 1)], s_sem.at[3])
    arrived(recv_2.at[1], s_sem.at[3])
    arrived(recv_3.at[pl.ds(1, EXPERTS - 1)], s_sem.at[4])
    arrived(send_4.at[pl.ds(0, OFFSETS - Z)], s_sem.at[5])
    arrived(send_5.at[pl.ds(1, Z - 1)], s_sem.at[6])


def solution(mesh):
    assert mesh.shape["ep"] == Z * Y * X and mesh.shape["tp"] == 2

    def local(tokens, norm_gain, routing, route_weight, w_gate, w_up, w_down):
        rows, half = tokens.shape
        vmem = pl.BlockSpec(memory_space=pltpu.VMEM)
        far = pl.BlockSpec(memory_space=pl.ANY)
        dma = pltpu.SemaphoreType.DMA
        bf16, f32 = jnp.bfloat16, jnp.float32
        line_rows = OFFSETS * CAP
        rounds = dma((Z,))
        return pl.pallas_call(
            kernel,
            out_shape=pltpu.VMEM((rows, half), bf16),
            in_specs=[far] * 7,
            out_specs=vmem,
            scratch_shapes=[
                pltpu.VMEM((2, rows), jnp.int32),
                pltpu.VMEM((2, rows), f32),
                pltpu.VMEM((2, 1, half), f32),
                pltpu.VMEM(w_gate.shape, bf16),
                pltpu.VMEM(w_up.shape, bf16),
                pltpu.VMEM(w_down.shape, bf16),
                pltpu.VMEM(w_gate.shape[1:], bf16),
                pltpu.VMEM(w_up.shape[1:], bf16),
                pltpu.VMEM(w_down.shape[1:], bf16),
                pltpu.VMEM((Z, 4, Y * SLOTS), f32),
                pltpu.VMEM((OFFSETS, 4, Y * SLOTS), f32),
                pltpu.VMEM((Z, X, rows, half), bf16),
                pltpu.VMEM((Z, X, 4, 2 * rows), f32),
                pltpu.VMEM((Z, 2, Y, 2, X // 2, CAP, half), bf16),
                pltpu.VMEM((2, Z, X, Y, CAP, half), bf16),
                pltpu.VMEM((X, 2, line_rows, half), bf16),
                pltpu.VMEM((EXPERTS, line_rows, half), bf16),
                pltpu.VMEM((OFFSETS, SLOTS, half), bf16),
                pltpu.VMEM((OFFSETS, SLOTS, half), bf16),
                pltpu.VMEM((Z, rows, half), bf16),
                pltpu.VMEM((Z, rows, half), bf16),
                dma((4,)), dma((3,)), dma((3,)), dma((4,)), dma((4,)), dma((7,)),
                rounds, dma((Z, X)), dma((Z, X)), rounds, rounds, rounds, rounds,
            ],
            compiler_params=pltpu.CompilerParams(collective_id=0, has_side_effects=True),
            name="experts",
        )(tokens, norm_gain.reshape(1, half), routing.T, route_weight.T, w_gate, w_up, w_down)

    in_specs = (
        P("ep", "tp"), P("tp"), P("ep", None), P("ep", None),
        P("ep", None, "tp"), P("ep", None, "tp"), P("ep", None, "tp"),
    )
    return jax.shard_map(local, mesh=mesh, in_specs=in_specs, out_specs=P("ep", "tp"), check_vma=False)
```

```python
import functools

import jax
import jax.numpy as jnp
from jax import lax
from jax.experimental import pallas as pl
from jax.experimental.pallas import tpu as pltpu
from jax.sharding import PartitionSpec as P

CAP = 8
EPSILON = 1e-06
MESH = pl.DeviceIdType.MESH

Z, Y, X = 8, 4, 4
EXPERTS = 2 * X
SLOTS = EXPERTS * CAP // 2
OFFSETS = Z * Y
STEPS = (0, 1, 7, 2, 6, 3, 5, 4)
LINE = (2, 1, 3)
GATHER = (1, 3, 2)
COLUMN = (2, 1, 3)
ORDER = """
    G00 M0 G01 A00 G02 G03 G10 A01 A10 A20 G11 G12 A21 G13 A11 M1 M2 F0 A40 G21 A30 G20 A31 G23 F2 M3 M4 G22 A41
    G30 A60 G31 A50 F3 G33 A61 A51 G32 F4 M5 M6 A70 F6 A71 M7 C3 F5 C4 F7 C6 F1 E4 C5 C2 E3 E6 C7 E5 C1 H3 E7 C0
    E2 E1 E0 H4 H0 H6 H2 H5 H1 H7
"""


def kernel(
    tok_hbm, gain_hbm, routing_hbm, weight_hbm, wg_hbm, wu_hbm, wd_hbm, out_ref,
    routing, weight, gains, wg, wu, wd, give_g, give_u, give_d,
    meta_s, meta_r, blocks, tables, send_2, recv_2, send_3, recv_3, send_4, recv_4, send_5, recv_5,
    in_sem, own_sem, give_sem, far_send, far_recv, s_sem, meta_sem, block_sem, table_sem, sem_2, sem_3, sem_4, sem_5,
):
    me, core = lax.axis_index("ep"), lax.axis_index("tp")
    other = 1 - core
    z, y, x = me // (Y * X), me // X % Y, me % X
    tokens, half = blocks.shape[2:]
    place_of = {step: p for p, step in enumerate(STEPS)}

    def plane(step, dy, sign):
        if sign > 0:
            return ((z + step) % Z * Y + (y + dy) % Y) * X + x
        return ((z + Z - step) % Z * Y + (y + Y - dy) % Y) * X + x

    def line(dx, sign):
        return me - x + (x + (dx if sign > 0 else X - dx)) % X

    stores = ((wg_hbm, wg, give_g), (wu_hbm, wu, give_u), (wd_hbm, wd, give_d))
    inputs = ((routing_hbm, routing), (weight_hbm, weight), (tok_hbm, blocks.at[0, 0]), (gain_hbm, gains.at[core]))
    inputs = [pltpu.make_async_copy(src, dst, in_sem.at[i]) for i, (src, dst) in enumerate(inputs)]
    own = [
        pltpu.make_async_copy(src.at[core], dst.at[core], own_sem.at[i])
        for i, (src, dst, _) in enumerate(stores)
    ]
    give = [
        pltpu.make_async_copy(src.at[other], stage, give_sem.at[i])
        for i, (src, _, stage) in enumerate(stores)
    ]
    for copy in inputs:
        copy.start()

    barrier = pltpu.get_barrier_semaphore()
    near = [(plane(step, 0, 1), core) for step in sorted({1, 2 % Z, Z - 2, Z - 1} - {0})] + [(me, other)]
    near += [(plane(0, dy, 1), c) for dy in range(1, Y) for c in range(2)]
    near += [(line(dx, 1), c) for dx in range(1, X) for c in range(2)]
    for device in near:
        pl.semaphore_signal(barrier, inc=1, device_id=device, device_id_type=MESH)
    for copy in give + own:
        copy.start()

    row = lax.broadcasted_iota(jnp.int32, (tokens, tokens), 0)
    col = lax.broadcasted_iota(jnp.int32, (tokens, tokens), 1)
    before = (row < col).astype(jnp.float32).astype(jnp.bfloat16)
    names = lax.broadcasted_iota(jnp.int32, (OFFSETS * EXPERTS, tokens), 0)
    inputs[0].wait()
    picks = [routing[k:k + 1, :] for k in range(2)]
    group = picks[0] // EXPERTS
    dz = (group // Y - z + Z) % Z
    dy = (group % Y - y + Y) % Y
    place = jnp.where(dz <= Z // 2, jnp.maximum(2 * dz - 1, 0), 2 * (Z - dz)) * Y + dy
    hot = [(picks[k] == names).astype(jnp.float32) for k in range(2)]
    hot_place = (place == names[:OFFSETS]).astype(jnp.float32)
    both = jnp.concatenate([hot[0] + hot[1], hot_place], axis=0).astype(jnp.bfloat16)
    earlier = jnp.dot(both, before, preferred_element_type=jnp.float32)
    slot = jnp.sum(earlier[OFFSETS * EXPERTS:] * hot_place, axis=0, keepdims=True)
    spot = place.astype(jnp.float32) * SLOTS + slot
    ranks = [jnp.sum(earlier[:OFFSETS * EXPERTS] * hot[k], axis=0, keepdims=True) for k in range(2)]
    codes = [(picks[k] % EXPERTS * CAP + 1).astype(jnp.float32) + ranks[k] for k in range(2)]
    seats = [(picks[k] * CAP).astype(jnp.float32) + ranks[k] for k in range(2)]
    inputs[1].wait()
    rows = [spot] + codes + [weight[k:k + 1, :] for k in range(2)] + seats + [spot]
    columns = jnp.transpose(jnp.concatenate(rows, axis=0))
    slots = OFFSETS * SLOTS
    lanes = lax.broadcasted_iota(jnp.int32, (tokens, slots), 1)
    at_home = lanes == columns[:, 0:1].astype(jnp.int32)
    for q in range(4):
        values = jnp.sum(jnp.where(at_home, columns[:, q + 1:q + 2], 0.0), axis=0, keepdims=True)
        for p in range(Z):
            meta_s[p, q:q + 1, :] = values[:, p * Y * SLOTS:(p + 1) * Y * SLOTS]
    repeated = lax.broadcasted_iota(jnp.int32, (tokens, 2 * tokens), 1) % tokens
    repeated = repeated == lax.broadcasted_iota(jnp.int32, (tokens, 2 * tokens), 0)
    for k in range(3):
        values = jnp.where(repeated, columns[:, 5 + k:6 + k], 0.0)
        tables[0, 0, k:k + 1, :] = jnp.sum(values, axis=0, keepdims=True)
    tables[0, 0, 3:4, :] = jnp.zeros((1, 2 * tokens), jnp.float32)
    inputs[2].wait()
    inputs[3].wait()

    pl.semaphore_wait(barrier, len(near))

    def remote(src, dst, send, recv, peer, c):
        return pltpu.make_async_remote_copy(
            src_ref=src, dst_ref=dst, send_sem=send, recv_sem=recv,
            device_id=(peer, c), device_id_type=MESH,
        )

    def arrived(ref, sem):
        pltpu.make_async_copy(ref, ref, sem).wait()

    def pass_on(p, j, q, i, peer):
        remote(tables.at[p, j], tables.at[q, i], s_sem.at[0], table_sem.at[q, i], peer, core).start()
        remote(blocks.at[p, j], blocks.at[q, i], s_sem.at[1], block_sem.at[q, i], peer, core).start()

    up, down = plane(1, 0, 1), plane(1, 0, -1)
    middle = Z // 2

    def step_g(k, j):
        for p in sorted({place_of[k], place_of[(Z - k) % Z]}):
            chunk_here(p, j)
        if (k, j) == (1, 0) and middle > 2:
            return
        if k + 1 < middle or j < X // 2:
            pass_on(place_of[k], j, place_of[k + 1], j, up)
        if k + 1 < middle or j >= X // 2:
            pass_on(place_of[(Z - k) % Z], j, place_of[Z - k - 1], j, down)
        if (k, j) == (0, 0) and middle > 2:
            pass_on(0, 0, place_of[2], 0, plane(2, 0, 1))
            pass_on(0, 0, place_of[Z - 2], 0, plane(2, 0, -1))

    seen = {(0, 0)}

    def chunk_here(p, j):
        if (p, j) not in seen:
            seen.add((p, j))
            arrived(tables.at[p, j], table_sem.at[p, j])
            arrived(blocks.at[p, j], block_sem.at[p, j])

    for dx in GATHER:
        pass_on(0, 0, 0, dx, line(dx, 1))
    step_g(0, 0)
    def step_m(p):
        assert (place_of[(Z - STEPS[p]) % Z], 0) in seen
        for dy in range(Y):
            if p or dy:
                o, peer = p * Y + dy, plane(STEPS[p], dy, 1)
                remote(meta_s.at[p], meta_r.at[o], s_sem.at[2], meta_sem.at[p], peer, core).start()
            else:
                pltpu.make_async_copy(meta_s.at[0], meta_r.at[0], meta_sem.at[0]).start()

    step_m(0)

    gain_copy = remote(gains.at[core], gains.at[core], far_send.at[3], far_recv.at[3], me, other)
    gain_copy.start()
    for copy in give:
        copy.wait()
    far = [
        remote(stage, dst.at[core], far_send.at[i], far_recv.at[i], me, other)
        for i, (_, dst, stage) in enumerate(stores)
    ]
    for copy in far:
        copy.start()

    def codes_of(p):
        segment = lax.broadcasted_iota(jnp.int32, (4, Y * SLOTS), 1) // SLOTS
        table = jnp.zeros((4, Y * SLOTS), jnp.float32)
        for dy in range(Y):
            table = jnp.where(segment == dy, meta_r[p * Y + dy], table)
        return table

    def step_a(p, h):
        pair = X // 2
        for j in range(h * pair, h * pair + pair):
            chunk_here(p, j)
        at = pl.ds(h * pair, pair)
        spot_of = lax.broadcasted_iota(jnp.int32, (4, pair * tokens), 1) // tokens
        seat = jnp.zeros((4, pair * tokens), jnp.float32)
        for j in range(pair):
            seat = jnp.where(spot_of == j, tables[p, h * pair + j, :, :pair * tokens], seat)
        seat = seat.astype(jnp.int32)
        pick = seat // CAP
        group, expert = pick // EXPERTS, pick % EXPERTS
        dy = (group % Y - y + Y) % Y
        target = ((dy * 2 + expert % 2) * pair + spot_of) * CAP + seat % CAP
        target = jnp.where((group // Y == z) & (expert // 2 == x), target, -1)
        places = lax.broadcasted_iota(jnp.int32, (Y * 2 * pair * CAP, pair * tokens), 0)
        take = (places == target[0:1]) | (places == target[1:2])
        take = take.astype(jnp.float32).astype(jnp.bfloat16)
        source = blocks[p, h * pair:h * pair + pair].reshape(pair * tokens, half)
        chosen = jnp.dot(take, source, preferred_element_type=jnp.float32)
        send_2[p, h] = chosen.reshape(Y, 2, pair, CAP, half).astype(jnp.bfloat16)
        for dy in COLUMN:
            for c in range(2):
                remote(
                    send_2.at[p, h, dy, c], recv_2.at[core, p, at, dy], s_sem.at[3], sem_2.at[p], plane(0, dy, 1), c
                ).start()
        remote(send_2.at[p, h, 0, other], recv_2.at[core, p, at, 0], s_sem.at[3], sem_2.at[p], me, other).start()
        pltpu.make_async_copy(send_2.at[p, h, 0, core], recv_2.at[core, p, at, 0], sem_2.at[p]).start()

    ready = []

    def step_f(p):
        count = Y * CAP
        at = pl.ds(p * count, count)
        arrived(recv_2.at[:, p], sem_2.at[p])
        if not ready:
            gain_copy.wait()
        parts = [recv_2[h, p].astype(jnp.float32).reshape(X * count, half) for h in range(2)]
        squares = sum(jnp.sum(part * part, axis=1, keepdims=True) for part in parts)
        scale = lax.rsqrt(squares / (2 * half) + EPSILON)
        normed = jnp.concatenate(
            [(part * scale * gains[h]).astype(jnp.bfloat16) for h, part in enumerate(parts)], axis=1
        )
        if not ready:
            for copy in own + far[:2]:
                copy.wait()
        hidden = []
        for h in range(2):
            gate = jnp.dot(normed, wg[h], preferred_element_type=jnp.float32)
            up = jnp.dot(normed, wu[h], preferred_element_type=jnp.float32)
            hidden.append((jax.nn.silu(gate) * up).astype(jnp.bfloat16))
        hidden = jnp.concatenate(hidden, axis=1)
        if not ready:
            far[2].wait()
            ready.append(True)
        for f in range(2):
            result = jnp.dot(hidden, wd[f], preferred_element_type=jnp.float32).astype(jnp.bfloat16)
            send_3[:, f, p * count:(p + 1) * count, :] = result.reshape(X, count, half)
        mine = x * 2 + core
        for dx in LINE:
            peer = line(dx, -1)
            for c in range(2):
                remote(
                    send_3.at[dx, c, at], recv_3.at[mine, at], s_sem.at[4], sem_3.at[p], peer, c
                ).start()
        remote(send_3.at[0, other, at], recv_3.at[mine, at], s_sem.at[4], sem_3.at[p], me, other).start()
        pltpu.make_async_copy(send_3.at[0, core, at], recv_3.at[mine, at], sem_3.at[p]).start()

    def step_c(p):
        arrived(meta_r.at[pl.ds(p * Y, Y)], meta_sem.at[p])
        table = codes_of(p)
        table = jnp.transpose(jnp.concatenate([table, jnp.zeros_like(table)], axis=0))
        block = lax.broadcasted_iota(jnp.int32, (Y * SLOTS, 1), 0) // SLOTS
        places = lax.broadcasted_iota(jnp.int32, (Y * SLOTS, EXPERTS * Y * CAP), 1)
        take = []
        for k in range(2):
            code = table[:, k:k + 1].astype(jnp.int32) - 1
            code = (code >> 3) * (Y * CAP) + block * CAP + (code & 7)
            take.append((places == code).astype(jnp.float32).astype(jnp.bfloat16))
        at = pl.ds(p * Y * CAP, Y * CAP)
        arrived(recv_3.at[:, at], sem_3.at[p])
        source = recv_3[:, p * Y * CAP:(p + 1) * Y * CAP, :].reshape(EXPERTS * Y * CAP, half)
        total = 0.0
        for k in range(2):
            total = total + table[:, 2 + k:3 + k] * jnp.dot(take[k], source, preferred_element_type=jnp.float32)
        send_4[p * Y:(p + 1) * Y] = total.astype(jnp.bfloat16).reshape(Y, SLOTS, half)
        for dy in COLUMN:
            o = p * Y + dy
            remote(send_4.at[o], recv_4.at[o], s_sem.at[5], sem_4.at[p], plane(0, dy, -1), core).start()
        pltpu.make_async_copy(send_4.at[p * Y], recv_4.at[p * Y], sem_4.at[p]).start()

    def step_e(p):
        table = tables[p, 0]
        table = jnp.transpose(jnp.concatenate([table, jnp.zeros_like(table)], axis=0))
        spot = table[:tokens, 2:3].astype(jnp.int32) - p * Y * SLOTS
        places = lax.broadcasted_iota(jnp.int32, (tokens, Y * SLOTS), 1)
        take = (places == spot).astype(jnp.float32).astype(jnp.bfloat16)
        arrived(recv_4.at[pl.ds(p * Y, Y)], sem_4.at[p])
        source = recv_4[p * Y:(p + 1) * Y].reshape(Y * SLOTS, half)
        send_5[p] = jnp.dot(take, source, preferred_element_type=jnp.float32).astype(jnp.bfloat16)
        if p:
            remote(send_5.at[p], recv_5.at[p], s_sem.at[6], sem_5.at[p], plane(STEPS[p], 0, -1), core).start()
        else:
            pltpu.make_async_copy(send_5.at[0], recv_5.at[0], sem_5.at[0]).start()

    def step_h(p):
        arrived(recv_5.at[p], sem_5.at[p])

    step_of = {"G": step_g, "M": step_m, "A": step_a, "F": step_f, "C": step_c, "E": step_e, "H": step_h}
    for name in ORDER.split():
        if name not in ("G00", "M0"):
            step_of[name[0]](*map(int, name[1:]))
    out_ref[...] = sum(recv_5[p].astype(jnp.float32) for p in range(Z)).astype(jnp.bfloat16)

    for at in ((pl.ds(1, Z - 1),), (0, pl.ds(1, X - 1))):
        arrived(tables.at[at], s_sem.at[0])
        arrived(blocks.at[at], s_sem.at[1])
    arrived(meta_r.at[pl.ds(1, OFFSETS - 1)], s_sem.at[2])
    arrived(recv_2.at[0, :, :, pl.ds(1, Y - 1)], s_sem.at[3])
    arrived(recv_2.at[1], s_sem.at[3])
    arrived(recv_3.at[pl.ds(1, EXPERTS - 1)], s_sem.at[4])
    arrived(send_4.at[pl.ds(0, OFFSETS - Z)], s_sem.at[5])
    arrived(send_5.at[pl.ds(1, Z - 1)], s_sem.at[6])


def solution(mesh):
    assert mesh.shape["ep"] == Z * Y * X and mesh.shape["tp"] == 2

    def local(tokens, norm_gain, routing, route_weight, w_gate, w_up, w_down):
        rows, half = tokens.shape
        vmem = pl.BlockSpec(memory_space=pltpu.VMEM)
        far = pl.BlockSpec(memory_space=pl.ANY)
        dma = pltpu.SemaphoreType.DMA
        bf16, f32 = jnp.bfloat16, jnp.float32
        line_rows = OFFSETS * CAP
        rounds = dma((Z,))
        return pl.pallas_call(
            kernel,
            out_shape=pltpu.VMEM((rows, half), bf16),
            in_specs=[far] * 7,
            out_specs=vmem,
            scratch_shapes=[
                pltpu.VMEM((2, rows), jnp.int32),
                pltpu.VMEM((2, rows), f32),
                pltpu.VMEM((2, 1, half), f32),
                pltpu.VMEM(w_gate.shape, bf16),
                pltpu.VMEM(w_up.shape, bf16),
                pltpu.VMEM(w_down.shape, bf16),
                pltpu.VMEM(w_gate.shape[1:], bf16),
                pltpu.VMEM(w_up.shape[1:], bf16),
                pltpu.VMEM(w_down.shape[1:], bf16),
                pltpu.VMEM((Z, 4, Y * SLOTS), f32),
                pltpu.VMEM((OFFSETS, 4, Y * SLOTS), f32),
                pltpu.VMEM((Z, X, rows, half), bf16),
                pltpu.VMEM((Z, X, 4, 2 * rows), f32),
                pltpu.VMEM((Z, 2, Y, 2, X // 2, CAP, half), bf16),
                pltpu.VMEM((2, Z, X, Y, CAP, half), bf16),
                pltpu.VMEM((X, 2, line_rows, half), bf16),
                pltpu.VMEM((EXPERTS, line_rows, half), bf16),
                pltpu.VMEM((OFFSETS, SLOTS, half), bf16),
                pltpu.VMEM((OFFSETS, SLOTS, half), bf16),
                pltpu.VMEM((Z, rows, half), bf16),
                pltpu.VMEM((Z, rows, half), bf16),
                dma((4,)), dma((3,)), dma((3,)), dma((4,)), dma((4,)), dma((7,)),
                rounds, dma((Z, X)), dma((Z, X)), rounds, rounds, rounds, rounds,
            ],
            compiler_params=pltpu.CompilerParams(collective_id=0, has_side_effects=True),
            name="experts",
        )(tokens, norm_gain.reshape(1, half), routing.T, route_weight.T, w_gate, w_up, w_down)

    in_specs = (
        P("ep", "tp"), P("tp"), P("ep", None), P("ep", None),
        P("ep", None, "tp"), P("ep", None, "tp"), P("ep", None, "tp"),
    )
    return jax.shard_map(local, mesh=mesh, in_specs=in_specs, out_specs=P("ep", "tp"), check_vma=False)
```

```python
import functools

import jax
import jax.numpy as jnp
from jax import lax
from jax.experimental import pallas as pl
from jax.experimental.pallas import tpu as pltpu
from jax.sharding import PartitionSpec as P

CAP = 8
EPSILON = 1e-06
MESH = pl.DeviceIdType.MESH

Z, Y, X = 8, 4, 4
EXPERTS = 2 * X
SLOTS = EXPERTS * CAP // 2
OFFSETS = Z * Y
STEPS = (0, 1, 7, 2, 6, 3, 5, 4)
LINE = (1, 3, 2)
GATHER = (1, 3, 2)
COLUMN = (2, 1, 3)
ORDER = """
    G00 A001 G01 A012 G02 G03 A201 G10 A101 A301 A401 M2 G11 A024 W G12 A112 A224 G13 A124 G20 G21 A312 A412 M1
    F0 G22 A324 A212 G23 A424 F1 A501 M3 M4 A601 G30 A512 A612 G32 F3 A624 M6 M5 G33 G31 F4 M0 A524 A701 F6 A712
    A724 F5 C3 C4 M7 C1 F7 C6 F2 C5 E4 E3 C0 E6 C7 E5 C2 E7 E2 E0 E1 H4 H3 H6 H0 H5 H2 H1 H7
"""


def kernel(
    tok_hbm, gain_hbm, routing_hbm, weight_hbm, wg_hbm, wu_hbm, wd_hbm, out_ref,
    routing, weight, gains, wg, wu, wd, give_g, give_u, give_d,
    meta_s, meta_r, blocks, tables, send_2, recv_2, send_3, recv_3, send_4, recv_4, send_5, recv_5,
    in_sem, own_sem, give_sem, far_send, far_recv, s_sem, meta_sem, block_sem, table_sem, sem_2, sem_3, sem_4, sem_5,
):
    me, core = lax.axis_index("ep"), lax.axis_index("tp")
    other = 1 - core
    z, y, x = me // (Y * X), me // X % Y, me % X
    tokens, half = blocks.shape[2:]
    place_of = {step: p for p, step in enumerate(STEPS)}

    def plane(step, dy, sign):
        if sign > 0:
            return ((z + step) % Z * Y + (y + dy) % Y) * X + x
        return ((z + Z - step) % Z * Y + (y + Y - dy) % Y) * X + x

    def line(dx, sign):
        return me - x + (x + (dx if sign > 0 else X - dx)) % X

    stores = ((wg_hbm, wg, give_g), (wu_hbm, wu, give_u), (wd_hbm, wd, give_d))
    inputs = ((routing_hbm, routing), (weight_hbm, weight), (tok_hbm, blocks.at[0, 0]), (gain_hbm, gains.at[core]))
    inputs = [pltpu.make_async_copy(src, dst, in_sem.at[i]) for i, (src, dst) in enumerate(inputs)]
    own = [
        pltpu.make_async_copy(src.at[core], dst.at[core], own_sem.at[i])
        for i, (src, dst, _) in enumerate(stores)
    ]
    give = [
        pltpu.make_async_copy(src.at[other], stage, give_sem.at[i])
        for i, (src, _, stage) in enumerate(stores)
    ]
    for copy in inputs:
        copy.start()

    barrier = pltpu.get_barrier_semaphore()
    near = [(plane(step, 0, 1), core) for step in sorted({1, 2 % Z, Z - 2, Z - 1} - {0})] + [(me, other)]
    near += [(plane(0, dy, 1), c) for dy in range(1, Y) for c in range(2)]
    near += [(line(dx, 1), c) for dx in range(1, X) for c in range(2)]
    for device in near:
        pl.semaphore_signal(barrier, inc=1, device_id=device, device_id_type=MESH)
    for copy in give + own:
        copy.start()

    row = lax.broadcasted_iota(jnp.int32, (tokens, tokens), 0)
    col = lax.broadcasted_iota(jnp.int32, (tokens, tokens), 1)
    before = (row < col).astype(jnp.float32).astype(jnp.bfloat16)
    names = lax.broadcasted_iota(jnp.int32, (OFFSETS * EXPERTS, tokens), 0)
    inputs[0].wait()
    picks = [routing[k:k + 1, :] for k in range(2)]
    group = picks[0] // EXPERTS
    dz = (group // Y - z + Z) % Z
    dy = (group % Y - y + Y) % Y
    place = jnp.where(dz <= Z // 2, jnp.maximum(2 * dz - 1, 0), 2 * (Z - dz)) * Y + dy
    hot = [(picks[k] == names).astype(jnp.float32) for k in range(2)]
    hot_place = (place == names[:OFFSETS]).astype(jnp.float32)
    both = jnp.concatenate([hot[0] + hot[1], hot_place], axis=0).astype(jnp.bfloat16)
    earlier = jnp.dot(both, before, preferred_element_type=jnp.float32)
    slot = jnp.sum(earlier[OFFSETS * EXPERTS:] * hot_place, axis=0, keepdims=True)
    spot = place.astype(jnp.float32) * SLOTS + slot
    ranks = [jnp.sum(earlier[:OFFSETS * EXPERTS] * hot[k], axis=0, keepdims=True) for k in range(2)]
    codes = [(picks[k] % EXPERTS * CAP + 1).astype(jnp.float32) + ranks[k] for k in range(2)]
    seats = [(picks[k] * CAP).astype(jnp.float32) + ranks[k] for k in range(2)]
    inputs[1].wait()
    rows = [spot] + codes + [weight[k:k + 1, :] for k in range(2)] + seats + [spot]
    columns = jnp.transpose(jnp.concatenate(rows, axis=0))
    slots = OFFSETS * SLOTS
    lanes = lax.broadcasted_iota(jnp.int32, (tokens, slots), 1)
    at_home = lanes == columns[:, 0:1].astype(jnp.int32)
    for q in range(4):
        values = jnp.sum(jnp.where(at_home, columns[:, q + 1:q + 2], 0.0), axis=0, keepdims=True)
        for p in range(Z):
            meta_s[p, q:q + 1, :] = values[:, p * Y * SLOTS:(p + 1) * Y * SLOTS]
    repeated = lax.broadcasted_iota(jnp.int32, (tokens, 2 * tokens), 1) % tokens
    repeated = repeated == lax.broadcasted_iota(jnp.int32, (tokens, 2 * tokens), 0)
    for k in range(3):
        values = jnp.where(repeated, columns[:, 5 + k:6 + k], 0.0)
        tables[0, 0, k:k + 1, :] = jnp.sum(values, axis=0, keepdims=True)
    tables[0, 0, 3:4, :] = jnp.zeros((1, 2 * tokens), jnp.float32)
    inputs[2].wait()
    inputs[3].wait()

    pl.semaphore_wait(barrier, len(near))

    def remote(src, dst, send, recv, peer, c):
        return pltpu.make_async_remote_copy(
            src_ref=src, dst_ref=dst, send_sem=send, recv_sem=recv,
            device_id=(peer, c), device_id_type=MESH,
        )

    def arrived(ref, sem):
        pltpu.make_async_copy(ref, ref, sem).wait()

    def pass_on(p, j, q, i, peer):
        remote(tables.at[p, j], tables.at[q, i], s_sem.at[0], table_sem.at[q, i], peer, core).start()
        remote(blocks.at[p, j], blocks.at[q, i], s_sem.at[1], block_sem.at[q, i], peer, core).start()

    up, down = plane(1, 0, 1), plane(1, 0, -1)
    middle = Z // 2

    def step_g(k, j):
        for p in sorted({place_of[k], place_of[(Z - k) % Z]}):
            chunk_here(p, j)
        if (k, j) == (1, 0) and middle > 2:
            return
        if k + 1 < middle or j < X // 2:
            pass_on(place_of[k], j, place_of[k + 1], j, up)
        if k + 1 < middle or j >= X // 2:
            pass_on(place_of[(Z - k) % Z], j, place_of[Z - k - 1], j, down)
        if (k, j) == (0, 0) and middle > 2:
            pass_on(0, 0, place_of[2], 0, plane(2, 0, 1))
            pass_on(0, 0, place_of[Z - 2], 0, plane(2, 0, -1))

    seen = {(0, 0)}

    def chunk_here(p, j):
        if (p, j) not in seen:
            seen.add((p, j))
            arrived(tables.at[p, j], table_sem.at[p, j])
            arrived(blocks.at[p, j], block_sem.at[p, j])

    for dx in GATHER:
        pass_on(0, 0, 0, dx, line(dx, 1))
    step_g(0, 0)
    def step_m(p):
        assert (place_of[(Z - STEPS[p]) % Z], 0) in seen
        for dy in range(Y):
            if p or dy:
                o, peer = p * Y + dy, plane(STEPS[p], dy, 1)
                remote(meta_s.at[p], meta_r.at[o], s_sem.at[2], meta_sem.at[p], peer, core).start()
            else:
                pltpu.make_async_copy(meta_s.at[0], meta_r.at[0], meta_sem.at[0]).start()

    step_m(0)

    gain_copy = remote(gains.at[core], gains.at[core], far_send.at[3], far_recv.at[3], me, other)
    gain_copy.start()
    far = [
        remote(stage, dst.at[core], far_send.at[i], far_recv.at[i], me, other)
        for i, (_, dst, stage) in enumerate(stores)
    ]

    def step_w():
        for copy in give:
            copy.wait()
        for copy in far:
            copy.start()

    def codes_of(p):
        segment = lax.broadcasted_iota(jnp.int32, (4, Y * SLOTS), 1) // SLOTS
        table = jnp.zeros((4, Y * SLOTS), jnp.float32)
        for dy in range(Y):
            table = jnp.where(segment == dy, meta_r[p * Y + dy], table)
        return table

    def step_a(p, first, last):
        count = last - first
        for j in range(first, last):
            chunk_here(p, j)
        at = pl.ds(first, count)
        spot_of = lax.broadcasted_iota(jnp.int32, (4, count * tokens), 1) // tokens
        seat = jnp.zeros((4, count * tokens), jnp.float32)
        for j in range(count):
            seat = jnp.where(spot_of == j, tables[p, first + j, :, :count * tokens], seat)
        seat = seat.astype(jnp.int32)
        pick = seat // CAP
        group, expert = pick // EXPERTS, pick % EXPERTS
        dy = (group % Y - y + Y) % Y
        target = ((spot_of * Y + dy) * 2 + expert % 2) * CAP + seat % CAP
        target = jnp.where((group // Y == z) & (expert // 2 == x), target, -1)
        places = lax.broadcasted_iota(jnp.int32, (count * Y * 2 * CAP, count * tokens), 0)
        take = (places == target[0:1]) | (places == target[1:2])
        take = take.astype(jnp.float32).astype(jnp.bfloat16)
        source = blocks[p, first:last].reshape(count * tokens, half)
        chosen = jnp.dot(take, source, preferred_element_type=jnp.float32)
        send_2[p, first:last] = chosen.reshape(count, Y, 2, CAP, half).astype(jnp.bfloat16)
        for dy in COLUMN:
            for c in range(2):
                remote(
                    send_2.at[p, at, dy, c], recv_2.at[core, p, at, dy], s_sem.at[3], sem_2.at[p], plane(0, dy, 1), c
                ).start()
        remote(send_2.at[p, at, 0, other], recv_2.at[core, p, at, 0], s_sem.at[3], sem_2.at[p], me, other).start()
        pltpu.make_async_copy(send_2.at[p, at, 0, core], recv_2.at[core, p, at, 0], sem_2.at[p]).start()

    ready = []

    def step_f(p):
        count = Y * CAP
        at = pl.ds(p * count, count)
        arrived(recv_2.at[:, p], sem_2.at[p])
        if not ready:
            gain_copy.wait()
        parts = [recv_2[h, p].astype(jnp.float32).reshape(X * count, half) for h in range(2)]
        squares = sum(jnp.sum(part * part, axis=1, keepdims=True) for part in parts)
        scale = lax.rsqrt(squares / (2 * half) + EPSILON)
        normed = jnp.concatenate(
            [(part * scale * gains[h]).astype(jnp.bfloat16) for h, part in enumerate(parts)], axis=1
        )
        if not ready:
            for copy in own + far[:2]:
                copy.wait()
        hidden = []
        for h in range(2):
            gate = jnp.dot(normed, wg[h], preferred_element_type=jnp.float32)
            up = jnp.dot(normed, wu[h], preferred_element_type=jnp.float32)
            hidden.append((jax.nn.silu(gate) * up).astype(jnp.bfloat16))
        hidden = jnp.concatenate(hidden, axis=1)
        if not ready:
            far[2].wait()
            ready.append(True)
        for f in range(2):
            result = jnp.dot(hidden, wd[f], preferred_element_type=jnp.float32).astype(jnp.bfloat16)
            send_3[:, f, p * count:(p + 1) * count, :] = result.reshape(X, count, half)
        mine = x * 2 + core
        for dx in LINE:
            peer = line(dx, -1)
            for c in range(2):
                remote(
                    send_3.at[dx, c, at], recv_3.at[mine, at], s_sem.at[4], sem_3.at[p], peer, c
                ).start()
        remote(send_3.at[0, other, at], recv_3.at[mine, at], s_sem.at[4], sem_3.at[p], me, other).start()
        pltpu.make_async_copy(send_3.at[0, core, at], recv_3.at[mine, at], sem_3.at[p]).start()

    def step_c(p):
        arrived(meta_r.at[pl.ds(p * Y, Y)], meta_sem.at[p])
        table = codes_of(p)
        table = jnp.transpose(jnp.concatenate([table, jnp.zeros_like(table)], axis=0))
        block = lax.broadcasted_iota(jnp.int32, (Y * SLOTS, 1), 0) // SLOTS
        places = lax.broadcasted_iota(jnp.int32, (Y * SLOTS, EXPERTS * Y * CAP), 1)
        take = []
        for k in range(2):
            code = table[:, k:k + 1].astype(jnp.int32) - 1
            code = (code >> 3) * (Y * CAP) + block * CAP + (code & 7)
            take.append((places == code).astype(jnp.float32).astype(jnp.bfloat16))
        at = pl.ds(p * Y * CAP, Y * CAP)
        arrived(recv_3.at[:, at], sem_3.at[p])
        source = recv_3[:, p * Y * CAP:(p + 1) * Y * CAP, :].reshape(EXPERTS * Y * CAP, half)
        total = 0.0
        for k in range(2):
            total = total + table[:, 2 + k:3 + k] * jnp.dot(take[k], source, preferred_element_type=jnp.float32)
        send_4[p * Y:(p + 1) * Y] = total.astype(jnp.bfloat16).reshape(Y, SLOTS, half)
        for dy in COLUMN:
            o = p * Y + dy
            remote(send_4.at[o], recv_4.at[o], s_sem.at[5], sem_4.at[p], plane(0, dy, -1), core).start()
        pltpu.make_async_copy(send_4.at[p * Y], recv_4.at[p * Y], sem_4.at[p]).start()

    def step_e(p):
        table = tables[p, 0]
        table = jnp.transpose(jnp.concatenate([table, jnp.zeros_like(table)], axis=0))
        spot = table[:tokens, 2:3].astype(jnp.int32) - p * Y * SLOTS
        places = lax.broadcasted_iota(jnp.int32, (tokens, Y * SLOTS), 1)
        take = (places == spot).astype(jnp.float32).astype(jnp.bfloat16)
        arrived(recv_4.at[pl.ds(p * Y, Y)], sem_4.at[p])
        source = recv_4[p * Y:(p + 1) * Y].reshape(Y * SLOTS, half)
        send_5[p] = jnp.dot(take, source, preferred_element_type=jnp.float32).astype(jnp.bfloat16)
        if p:
            remote(send_5.at[p], recv_5.at[p], s_sem.at[6], sem_5.at[p], plane(STEPS[p], 0, -1), core).start()
        else:
            pltpu.make_async_copy(send_5.at[0], recv_5.at[0], sem_5.at[0]).start()

    sums = []
    last = int(ORDER.split()[-1][1:])

    def step_h(p):
        if p == last:
            sums.append(sum(recv_5[q].astype(jnp.float32) for q in range(Z) if q != last))
        arrived(recv_5.at[p], sem_5.at[p])

    step_of = {"W": step_w, "G": step_g, "M": step_m, "A": step_a, "F": step_f, "C": step_c, "E": step_e, "H": step_h}
    for name in ORDER.split():
        if name not in ("G00", "M0"):
            step_of[name[0]](*map(int, name[1:]))
    out_ref[...] = (sums[0] + recv_5[last].astype(jnp.float32)).astype(jnp.bfloat16)

    for at in ((pl.ds(1, Z - 1),), (0, pl.ds(1, X - 1))):
        arrived(tables.at[at], s_sem.at[0])
        arrived(blocks.at[at], s_sem.at[1])
    arrived(meta_r.at[pl.ds(1, OFFSETS - 1)], s_sem.at[2])
    arrived(recv_2.at[0, :, :, pl.ds(1, Y - 1)], s_sem.at[3])
    arrived(recv_2.at[1], s_sem.at[3])
    arrived(recv_3.at[pl.ds(1, EXPERTS - 1)], s_sem.at[4])
    arrived(send_4.at[pl.ds(0, OFFSETS - Z)], s_sem.at[5])
    arrived(send_5.at[pl.ds(1, Z - 1)], s_sem.at[6])


def solution(mesh):
    assert mesh.shape["ep"] == Z * Y * X and mesh.shape["tp"] == 2

    def local(tokens, norm_gain, routing, route_weight, w_gate, w_up, w_down):
        rows, half = tokens.shape
        vmem = pl.BlockSpec(memory_space=pltpu.VMEM)
        far = pl.BlockSpec(memory_space=pl.ANY)
        dma = pltpu.SemaphoreType.DMA
        bf16, f32 = jnp.bfloat16, jnp.float32
        line_rows = OFFSETS * CAP
        rounds = dma((Z,))
        return pl.pallas_call(
            kernel,
            out_shape=pltpu.VMEM((rows, half), bf16),
            in_specs=[far] * 7,
            out_specs=vmem,
            scratch_shapes=[
                pltpu.VMEM((2, rows), jnp.int32),
                pltpu.VMEM((2, rows), f32),
                pltpu.VMEM((2, 1, half), f32),
                pltpu.VMEM(w_gate.shape, bf16),
                pltpu.VMEM(w_up.shape, bf16),
                pltpu.VMEM(w_down.shape, bf16),
                pltpu.VMEM(w_gate.shape[1:], bf16),
                pltpu.VMEM(w_up.shape[1:], bf16),
                pltpu.VMEM(w_down.shape[1:], bf16),
                pltpu.VMEM((Z, 4, Y * SLOTS), f32),
                pltpu.VMEM((OFFSETS, 4, Y * SLOTS), f32),
                pltpu.VMEM((Z, X, rows, half), bf16),
                pltpu.VMEM((Z, X, 4, 2 * rows), f32),
                pltpu.VMEM((Z, X, Y, 2, CAP, half), bf16),
                pltpu.VMEM((2, Z, X, Y, CAP, half), bf16),
                pltpu.VMEM((X, 2, line_rows, half), bf16),
                pltpu.VMEM((EXPERTS, line_rows, half), bf16),
                pltpu.VMEM((OFFSETS, SLOTS, half), bf16),
                pltpu.VMEM((OFFSETS, SLOTS, half), bf16),
                pltpu.VMEM((Z, rows, half), bf16),
                pltpu.VMEM((Z, rows, half), bf16),
                dma((4,)), dma((3,)), dma((3,)), dma((4,)), dma((4,)), dma((7,)),
                rounds, dma((Z, X)), dma((Z, X)), rounds, rounds, rounds, rounds,
            ],
            compiler_params=pltpu.CompilerParams(collective_id=0, has_side_effects=True),
            name="experts",
        )(tokens, norm_gain.reshape(1, half), routing.T, route_weight.T, w_gate, w_up, w_down)

    in_specs = (
        P("ep", "tp"), P("tp"), P("ep", None), P("ep", None),
        P("ep", None, "tp"), P("ep", None, "tp"), P("ep", None, "tp"),
    )
    return jax.shard_map(local, mesh=mesh, in_specs=in_specs, out_specs=P("ep", "tp"), check_vma=False)
```

```python
import functools

import jax
import jax.numpy as jnp
from jax import lax
from jax.experimental import pallas as pl
from jax.experimental.pallas import tpu as pltpu
from jax.sharding import PartitionSpec as P

CAP = 8
EPSILON = 1e-06
MESH = pl.DeviceIdType.MESH

Z, Y, X = 8, 4, 4
EXPERTS = 2 * X
SLOTS = EXPERTS * CAP // 2
OFFSETS = Z * Y
STEPS = (0, 1, 7, 2, 6, 3, 5, 4)
LINE = (2, 1, 3)
GATHER = (1, 3, 2)
COLUMN = (2, 1, 3)
ORDER = (
    "G00", "M0", "G01", "A00", "G02", "G03", "G10", "A01", "A10", "A20", "G11", "G12", "A21", "G13", "A11",
    "M1", "M2", "F0", "A40", "G21", "A30", "G20", "A31", "G23", "F2", "M3", "M4", "G22", "A41", "G30", "A60",
    "G31", "A50", "F3", "G33", "A61", "A51", "G32", "F4", "M5", "M6", "A70", "F6", "A71", "M7", "C3", "F5",
    "C4", "F7", "C6", "F1", "E4", "C5", "C2", "E3", "E6", "C7", "E5", "C1", "H3", "E7", "C0", "E2", "E1", "E0",
    "H4", "H0", "H6", "H2", "H5", "H1", "H7",
)


def kernel(
    tok_hbm, gain_hbm, routing_hbm, weight_hbm, wg_hbm, wu_hbm, wd_hbm, out_ref,
    routing, weight, gains, wg, wu, wd, give_g, give_u, give_d,
    meta_s, meta_r, blocks, tables, send_2, recv_2, send_3, recv_3, send_4, recv_4, send_5, recv_5,
    in_sem, own_sem, give_sem, far_send, far_recv, s_sem, meta_sem, block_sem, table_sem, sem_2, sem_3, sem_4, sem_5,
):
    me, core = lax.axis_index("ep"), lax.axis_index("tp")
    other = 1 - core
    z, y, x = me // (Y * X), me // X % Y, me % X
    tokens, half = blocks.shape[2:]
    place_of = {step: p for p, step in enumerate(STEPS)}

    def plane(step, dy, sign):
        if sign > 0:
            return ((z + step) % Z * Y + (y + dy) % Y) * X + x
        return ((z + Z - step) % Z * Y + (y + Y - dy) % Y) * X + x

    def line(dx, sign):
        return me - x + (x + (dx if sign > 0 else X - dx)) % X

    stores = ((wg_hbm, wg, give_g), (wu_hbm, wu, give_u), (wd_hbm, wd, give_d))
    inputs = ((routing_hbm, routing), (weight_hbm, weight), (tok_hbm, blocks.at[0, 0]), (gain_hbm, gains.at[core]))
    inputs = [pltpu.make_async_copy(src, dst, in_sem.at[i]) for i, (src, dst) in enumerate(inputs)]
    own = [
        pltpu.make_async_copy(src.at[core], dst.at[core], own_sem.at[i])
        for i, (src, dst, _) in enumerate(stores)
    ]
    give = [
        pltpu.make_async_copy(src.at[other], stage, give_sem.at[i])
        for i, (src, _, stage) in enumerate(stores)
    ]
    for copy in inputs:
        copy.start()

    barrier = pltpu.get_barrier_semaphore()
    near = [(plane(step, 0, 1), core) for step in sorted({1, 2 % Z, Z - 2, Z - 1} - {0})] + [(me, other)]
    near += [(plane(0, dy, 1), c) for dy in range(1, Y) for c in range(2)]
    near += [(line(dx, 1), c) for dx in range(1, X) for c in range(2)]
    for device in near:
        pl.semaphore_signal(barrier, inc=1, device_id=device, device_id_type=MESH)
    for copy in give + own:
        copy.start()

    row = lax.broadcasted_iota(jnp.int32, (tokens, tokens), 0)
    col = lax.broadcasted_iota(jnp.int32, (tokens, tokens), 1)
    before = (row < col).astype(jnp.float32).astype(jnp.bfloat16)
    names = lax.broadcasted_iota(jnp.int32, (OFFSETS * EXPERTS, tokens), 0)
    inputs[0].wait()
    picks = [routing[k:k + 1, :] for k in range(2)]
    group = picks[0] // EXPERTS
    dz = (group // Y - z + Z) % Z
    dy = (group % Y - y + Y) % Y
    place = jnp.where(dz <= Z // 2, jnp.maximum(2 * dz - 1, 0), 2 * (Z - dz)) * Y + dy
    hot = [(picks[k] == names).astype(jnp.float32) for k in range(2)]
    hot_place = (place == names[:OFFSETS]).astype(jnp.float32)
    both = jnp.concatenate([hot[0] + hot[1], hot_place], axis=0).astype(jnp.bfloat16)
    earlier = jnp.dot(both, before, preferred_element_type=jnp.float32)
    slot = jnp.sum(earlier[OFFSETS * EXPERTS:] * hot_place, axis=0, keepdims=True)
    spot = place.astype(jnp.float32) * SLOTS + slot
    ranks = [jnp.sum(earlier[:OFFSETS * EXPERTS] * hot[k], axis=0, keepdims=True) for k in range(2)]
    codes = [(picks[k] % EXPERTS * CAP + 1).astype(jnp.float32) + ranks[k] for k in range(2)]
    seats = [(picks[k] * CAP).astype(jnp.float32) + ranks[k] for k in range(2)]
    inputs[1].wait()
    rows = [spot] + codes + [weight[k:k + 1, :] for k in range(2)] + seats + [spot]
    columns = jnp.transpose(jnp.concatenate(rows, axis=0))
    slots = OFFSETS * SLOTS
    lanes = lax.broadcasted_iota(jnp.int32, (tokens, slots), 1)
    at_home = lanes == columns[:, 0:1].astype(jnp.int32)
    for q in range(4):
        values = jnp.sum(jnp.where(at_home, columns[:, q + 1:q + 2], 0.0), axis=0, keepdims=True)
        for p in range(Z):
            meta_s[p, q:q + 1, :] = values[:, p * Y * SLOTS:(p + 1) * Y * SLOTS]
    repeated = lax.broadcasted_iota(jnp.int32, (tokens, 2 * tokens), 1) % tokens
    repeated = repeated == lax.broadcasted_iota(jnp.int32, (tokens, 2 * tokens), 0)
    for k in range(3):
        values = jnp.where(repeated, columns[:, 5 + k:6 + k], 0.0)
        tables[0, 0, k:k + 1, :] = jnp.sum(values, axis=0, keepdims=True)
    tables[0, 0, 3:4, :] = jnp.zeros((1, 2 * tokens), jnp.float32)
    inputs[2].wait()
    inputs[3].wait()

    pl.semaphore_wait(barrier, len(near))

    def remote(src, dst, send, recv, peer, c):
        return pltpu.make_async_remote_copy(
            src_ref=src, dst_ref=dst, send_sem=send, recv_sem=recv,
            device_id=(peer, c), device_id_type=MESH,
        )

    def arrived(ref, sem):
        pltpu.make_async_copy(ref, ref, sem).wait()

    def pass_on(p, j, q, i, peer):
        remote(tables.at[p, j], tables.at[q, i], s_sem.at[0], table_sem.at[q, i], peer, core).start()
        remote(blocks.at[p, j], blocks.at[q, i], s_sem.at[1], block_sem.at[q, i], peer, core).start()

    up, down = plane(1, 0, 1), plane(1, 0, -1)
    middle = Z // 2

    def step_g(k, j):
        for p in sorted({place_of[k], place_of[(Z - k) % Z]}):
            chunk_here(p, j)
        if (k, j) == (1, 0) and middle > 2:
            return
        if k + 1 < middle or j < X // 2:
            pass_on(place_of[k], j, place_of[k + 1], j, up)
        if k + 1 < middle or j >= X // 2:
            pass_on(place_of[(Z - k) % Z], j, place_of[Z - k - 1], j, down)
        if (k, j) == (0, 0) and middle > 2:
            pass_on(0, 0, place_of[2], 0, plane(2, 0, 1))
            pass_on(0, 0, place_of[Z - 2], 0, plane(2, 0, -1))

    seen = {(0, 0)}

    def chunk_here(p, j):
        if (p, j) not in seen:
            seen.add((p, j))
            arrived(tables.at[p, j], table_sem.at[p, j])
            arrived(blocks.at[p, j], block_sem.at[p, j])

    for dx in GATHER:
        pass_on(0, 0, 0, dx, line(dx, 1))
    step_g(0, 0)
    def step_m(p):
        assert (place_of[(Z - STEPS[p]) % Z], 0) in seen
        for dy in range(Y):
            if p or dy:
                o, peer = p * Y + dy, plane(STEPS[p], dy, 1)
                remote(meta_s.at[p], meta_r.at[o], s_sem.at[2], meta_sem.at[p], peer, core).start()
            else:
                pltpu.make_async_copy(meta_s.at[0], meta_r.at[0], meta_sem.at[0]).start()

    step_m(0)

    gain_copy = remote(gains.at[core], gains.at[core], far_send.at[3], far_recv.at[3], me, other)
    gain_copy.start()
    for copy in give:
        copy.wait()
    far = [
        remote(stage, dst.at[core], far_send.at[i], far_recv.at[i], me, other)
        for i, (_, dst, stage) in enumerate(stores)
    ]
    for copy in far:
        copy.start()

    def codes_of(p):
        segment = lax.broadcasted_iota(jnp.int32, (4, Y * SLOTS), 1) // SLOTS
        table = jnp.zeros((4, Y * SLOTS), jnp.float32)
        for dy in range(Y):
            table = jnp.where(segment == dy, meta_r[p * Y + dy], table)
        return table

    def step_a(p, h):
        pair = X // 2
        for j in range(h * pair, h * pair + pair):
            chunk_here(p, j)
        at = pl.ds(h * pair, pair)
        spot_of = lax.broadcasted_iota(jnp.int32, (4, pair * tokens), 1) // tokens
        seat = jnp.zeros((4, pair * tokens), jnp.float32)
        for j in range(pair):
            seat = jnp.where(spot_of == j, tables[p, h * pair + j, :, :pair * tokens], seat)
        seat = seat.astype(jnp.int32)
        pick = seat // CAP
        group, expert = pick // EXPERTS, pick % EXPERTS
        dy = (group % Y - y + Y) % Y
        target = ((dy * 2 + expert % 2) * pair + spot_of) * CAP + seat % CAP
        target = jnp.where((group // Y == z) & (expert // 2 == x), target, -1)
        places = lax.broadcasted_iota(jnp.int32, (Y * 2 * pair * CAP, pair * tokens), 0)
        take = (places == target[0:1]) | (places == target[1:2])
        take = take.astype(jnp.float32).astype(jnp.bfloat16)
        source = blocks[p, h * pair:h * pair + pair].reshape(pair * tokens, half)
        chosen = jnp.dot(take, source, preferred_element_type=jnp.float32)
        send_2[p, h] = chosen.reshape(Y, 2, pair, CAP, half).astype(jnp.bfloat16)
        for dy in COLUMN:
            for c in range(2):
                remote(
                    send_2.at[p, h, dy, c], recv_2.at[core, p, at, dy], s_sem.at[3], sem_2.at[p], plane(0, dy, 1), c
                ).start()
        remote(send_2.at[p, h, 0, other], recv_2.at[core, p, at, 0], s_sem.at[3], sem_2.at[p], me, other).start()
        pltpu.make_async_copy(send_2.at[p, h, 0, core], recv_2.at[core, p, at, 0], sem_2.at[p]).start()

    ready = []

    def step_f(p):
        count = Y * CAP
        at = pl.ds(p * count, count)
        arrived(recv_2.at[:, p], sem_2.at[p])
        if not ready:
            gain_copy.wait()
        parts = [recv_2[h, p].astype(jnp.float32).reshape(X * count, half) for h in range(2)]
        squares = sum(jnp.sum(part * part, axis=1, keepdims=True) for part in parts)
        scale = lax.rsqrt(squares / (2 * half) + EPSILON)
        normed = jnp.concatenate(
            [(part * scale * gains[h]).astype(jnp.bfloat16) for h, part in enumerate(parts)], axis=1
        )
        if not ready:
            for copy in own + far[:2]:
                copy.wait()
        hidden = []
        for h in range(2):
            gate = jnp.dot(normed, wg[h], preferred_element_type=jnp.float32)
            up = jnp.dot(normed, wu[h], preferred_element_type=jnp.float32)
            hidden.append((jax.nn.silu(gate) * up).astype(jnp.bfloat16))
        hidden = jnp.concatenate(hidden, axis=1)
        if not ready:
            far[2].wait()
            ready.append(True)
        for f in range(2):
            result = jnp.dot(hidden, wd[f], preferred_element_type=jnp.float32).astype(jnp.bfloat16)
            send_3[:, f, p * count:(p + 1) * count, :] = result.reshape(X, count, half)
        mine = x * 2 + core
        for dx in LINE:
            peer = line(dx, -1)
            for c in range(2):
                remote(
                    send_3.at[dx, c, at], recv_3.at[mine, at], s_sem.at[4], sem_3.at[p], peer, c
                ).start()
        remote(send_3.at[0, other, at], recv_3.at[mine, at], s_sem.at[4], sem_3.at[p], me, other).start()
        pltpu.make_async_copy(send_3.at[0, core, at], recv_3.at[mine, at], sem_3.at[p]).start()

    def step_c(p):
        arrived(meta_r.at[pl.ds(p * Y, Y)], meta_sem.at[p])
        table = codes_of(p)
        table = jnp.transpose(jnp.concatenate([table, jnp.zeros_like(table)], axis=0))
        block = lax.broadcasted_iota(jnp.int32, (Y * SLOTS, 1), 0) // SLOTS
        places = lax.broadcasted_iota(jnp.int32, (Y * SLOTS, EXPERTS * Y * CAP), 1)
        take = []
        for k in range(2):
            code = table[:, k:k + 1].astype(jnp.int32) - 1
            code = (code >> 3) * (Y * CAP) + block * CAP + (code & 7)
            take.append((places == code).astype(jnp.float32).astype(jnp.bfloat16))
        at = pl.ds(p * Y * CAP, Y * CAP)
        arrived(recv_3.at[:, at], sem_3.at[p])
        source = recv_3[:, p * Y * CAP:(p + 1) * Y * CAP, :].reshape(EXPERTS * Y * CAP, half)
        total = 0.0
        for k in range(2):
            total = total + table[:, 2 + k:3 + k] * jnp.dot(take[k], source, preferred_element_type=jnp.float32)
        send_4[p * Y:(p + 1) * Y] = total.astype(jnp.bfloat16).reshape(Y, SLOTS, half)
        for dy in COLUMN:
            o = p * Y + dy
            remote(send_4.at[o], recv_4.at[o], s_sem.at[5], sem_4.at[p], plane(0, dy, -1), core).start()
        pltpu.make_async_copy(send_4.at[p * Y], recv_4.at[p * Y], sem_4.at[p]).start()

    def step_e(p):
        table = tables[p, 0]
        table = jnp.transpose(jnp.concatenate([table, jnp.zeros_like(table)], axis=0))
        spot = table[:tokens, 2:3].astype(jnp.int32) - p * Y * SLOTS
        places = lax.broadcasted_iota(jnp.int32, (tokens, Y * SLOTS), 1)
        take = (places == spot).astype(jnp.float32).astype(jnp.bfloat16)
        arrived(recv_4.at[pl.ds(p * Y, Y)], sem_4.at[p])
        source = recv_4[p * Y:(p + 1) * Y].reshape(Y * SLOTS, half)
        send_5[p] = jnp.dot(take, source, preferred_element_type=jnp.float32).astype(jnp.bfloat16)
        if p:
            remote(send_5.at[p], recv_5.at[p], s_sem.at[6], sem_5.at[p], plane(STEPS[p], 0, -1), core).start()
        else:
            pltpu.make_async_copy(send_5.at[0], recv_5.at[0], sem_5.at[0]).start()

    def step_h(p):
        arrived(recv_5.at[p], sem_5.at[p])

    step_of = {"G": step_g, "M": step_m, "A": step_a, "F": step_f, "C": step_c, "E": step_e, "H": step_h}
    for name in ORDER:
        if name not in ("G00", "M0"):
            step_of[name[0]](*map(int, name[1:]))
    out_ref[...] = sum(recv_5[p].astype(jnp.float32) for p in range(Z)).astype(jnp.bfloat16)

    for at in ((pl.ds(1, Z - 1),), (0, pl.ds(1, X - 1))):
        arrived(tables.at[at], s_sem.at[0])
        arrived(blocks.at[at], s_sem.at[1])
    arrived(meta_r.at[pl.ds(1, OFFSETS - 1)], s_sem.at[2])
    arrived(recv_2.at[0, :, :, pl.ds(1, Y - 1)], s_sem.at[3])
    arrived(recv_2.at[1], s_sem.at[3])
    arrived(recv_3.at[pl.ds(1, EXPERTS - 1)], s_sem.at[4])
    arrived(send_4.at[pl.ds(0, OFFSETS - Z)], s_sem.at[5])
    arrived(send_5.at[pl.ds(1, Z - 1)], s_sem.at[6])


def solution(mesh):
    assert mesh.shape["ep"] == Z * Y * X and mesh.shape["tp"] == 2

    def local(tokens, norm_gain, routing, route_weight, w_gate, w_up, w_down):
        rows, half = tokens.shape
        vmem = pl.BlockSpec(memory_space=pltpu.VMEM)
        far = pl.BlockSpec(memory_space=pl.ANY)
        dma = pltpu.SemaphoreType.DMA
        bf16, f32 = jnp.bfloat16, jnp.float32
        line_rows = OFFSETS * CAP
        rounds = dma((Z,))
        return pl.pallas_call(
            kernel,
            out_shape=pltpu.VMEM((rows, half), bf16),
            in_specs=[far] * 7,
            out_specs=vmem,
            scratch_shapes=[
                pltpu.VMEM((2, rows), jnp.int32),
                pltpu.VMEM((2, rows), f32),
                pltpu.VMEM((2, 1, half), f32),
                pltpu.VMEM(w_gate.shape, bf16),
                pltpu.VMEM(w_up.shape, bf16),
                pltpu.VMEM(w_down.shape, bf16),
                pltpu.VMEM(w_gate.shape[1:], bf16),
                pltpu.VMEM(w_up.shape[1:], bf16),
                pltpu.VMEM(w_down.shape[1:], bf16),
                pltpu.VMEM((Z, 4, Y * SLOTS), f32),
                pltpu.VMEM((OFFSETS, 4, Y * SLOTS), f32),
                pltpu.VMEM((Z, X, rows, half), bf16),
                pltpu.VMEM((Z, X, 4, 2 * rows), f32),
                pltpu.VMEM((Z, 2, Y, 2, X // 2, CAP, half), bf16),
                pltpu.VMEM((2, Z, X, Y, CAP, half), bf16),
                pltpu.VMEM((X, 2, line_rows, half), bf16),
                pltpu.VMEM((EXPERTS, line_rows, half), bf16),
                pltpu.VMEM((OFFSETS, SLOTS, half), bf16),
                pltpu.VMEM((OFFSETS, SLOTS, half), bf16),
                pltpu.VMEM((Z, rows, half), bf16),
                pltpu.VMEM((Z, rows, half), bf16),
                dma((4,)), dma((3,)), dma((3,)), dma((4,)), dma((4,)), dma((7,)),
                rounds, dma((Z, X)), dma((Z, X)), rounds, rounds, rounds, rounds,
            ],
            compiler_params=pltpu.CompilerParams(collective_id=0, has_side_effects=True),
            name="experts",
        )(tokens, norm_gain.reshape(1, half), routing.T, route_weight.T, w_gate, w_up, w_down)

    in_specs = (
        P("ep", "tp"), P("tp"), P("ep", None), P("ep", None),
        P("ep", None, "tp"), P("ep", None, "tp"), P("ep", None, "tp"),
    )
    return jax.shard_map(local, mesh=mesh, in_specs=in_specs, out_specs=P("ep", "tp"), check_vma=False)
```

```python
import functools

import jax
import jax.numpy as jnp
from jax import lax
from jax.experimental import pallas as pl
from jax.experimental.pallas import tpu as pltpu
from jax.sharding import PartitionSpec as P

CAP = 8
EPSILON = 1e-06
MESH = pl.DeviceIdType.MESH

Z, Y, X = 8, 4, 4
EXPERTS = 2 * X
SLOTS = EXPERTS * CAP // 2
OFFSETS = Z * Y
STEPS = (0, 1, 7, 2, 6, 3, 5, 4)
LINE = (1, 3, 2)
GATHER = (1, 3, 2)
COLUMN = (2, 1, 3)
ORDER = (
    "G00", "A001", "G01", "A012", "G02", "G03", "A201", "G10", "A101", "A301", "A401", "M2", "G11", "A024",
    "G12", "A112", "A224", "G13", "A124", "G20", "G21", "A312", "A412", "M1", "F0", "G22", "A324", "A212",
    "G23", "A424", "F1", "A501", "M3", "M4", "A601", "G30", "A512", "A612", "G32", "F3", "A624", "M6", "M5",
    "G33", "G31", "F4", "M0", "A524", "A701", "F6", "A712", "A724", "F5", "C3", "C4", "M7", "C1", "F7", "C6",
    "F2", "C5", "E4", "E3", "C0", "E6", "C7", "E5", "C2", "E7", "E2", "E0", "E1", "H4", "H3", "H6", "H0", "H5",
    "H2", "H1", "H7",
)


def kernel(
    tok_hbm, gain_hbm, routing_hbm, weight_hbm, wg_hbm, wu_hbm, wd_hbm, out_ref,
    routing, weight, gains, wg, wu, wd, give_g, give_u, give_d,
    meta_s, meta_r, blocks, tables, send_2, recv_2, send_3, recv_3, send_4, recv_4, send_5, recv_5,
    in_sem, own_sem, give_sem, far_send, far_recv, s_sem, meta_sem, block_sem, table_sem, sem_2, sem_3, sem_4, sem_5,
):
    me, core = lax.axis_index("ep"), lax.axis_index("tp")
    other = 1 - core
    z, y, x = me // (Y * X), me // X % Y, me % X
    tokens, half = blocks.shape[2:]
    place_of = {step: p for p, step in enumerate(STEPS)}

    def plane(step, dy, sign):
        if sign > 0:
            return ((z + step) % Z * Y + (y + dy) % Y) * X + x
        return ((z + Z - step) % Z * Y + (y + Y - dy) % Y) * X + x

    def line(dx, sign):
        return me - x + (x + (dx if sign > 0 else X - dx)) % X

    stores = ((wg_hbm, wg, give_g), (wu_hbm, wu, give_u), (wd_hbm, wd, give_d))
    inputs = ((routing_hbm, routing), (weight_hbm, weight), (tok_hbm, blocks.at[0, 0]), (gain_hbm, gains.at[core]))
    inputs = [pltpu.make_async_copy(src, dst, in_sem.at[i]) for i, (src, dst) in enumerate(inputs)]
    own = [
        pltpu.make_async_copy(src.at[core], dst.at[core], own_sem.at[i])
        for i, (src, dst, _) in enumerate(stores)
    ]
    give = [
        pltpu.make_async_copy(src.at[other], stage, give_sem.at[i])
        for i, (src, _, stage) in enumerate(stores)
    ]
    for copy in inputs:
        copy.start()

    barrier = pltpu.get_barrier_semaphore()
    near = [(plane(step, 0, 1), core) for step in sorted({1, 2 % Z, Z - 2, Z - 1} - {0})] + [(me, other)]
    near += [(plane(0, dy, 1), c) for dy in range(1, Y) for c in range(2)]
    near += [(line(dx, 1), c) for dx in range(1, X) for c in range(2)]
    for device in near:
        pl.semaphore_signal(barrier, inc=1, device_id=device, device_id_type=MESH)
    for copy in give + own:
        copy.start()

    row = lax.broadcasted_iota(jnp.int32, (tokens, tokens), 0)
    col = lax.broadcasted_iota(jnp.int32, (tokens, tokens), 1)
    before = (row < col).astype(jnp.float32).astype(jnp.bfloat16)
    names = lax.broadcasted_iota(jnp.int32, (OFFSETS * EXPERTS, tokens), 0)
    inputs[0].wait()
    picks = [routing[k:k + 1, :] for k in range(2)]
    group = picks[0] // EXPERTS
    dz = (group // Y - z + Z) % Z
    dy = (group % Y - y + Y) % Y
    place = jnp.where(dz <= Z // 2, jnp.maximum(2 * dz - 1, 0), 2 * (Z - dz)) * Y + dy
    hot = [(picks[k] == names).astype(jnp.float32) for k in range(2)]
    hot_place = (place == names[:OFFSETS]).astype(jnp.float32)
    both = jnp.concatenate([hot[0] + hot[1], hot_place], axis=0).astype(jnp.bfloat16)
    earlier = jnp.dot(both, before, preferred_element_type=jnp.float32)
    slot = jnp.sum(earlier[OFFSETS * EXPERTS:] * hot_place, axis=0, keepdims=True)
    spot = place.astype(jnp.float32) * SLOTS + slot
    ranks = [jnp.sum(earlier[:OFFSETS * EXPERTS] * hot[k], axis=0, keepdims=True) for k in range(2)]
    codes = [(picks[k] % EXPERTS * CAP + 1).astype(jnp.float32) + ranks[k] for k in range(2)]
    seats = [(picks[k] * CAP).astype(jnp.float32) + ranks[k] for k in range(2)]
    inputs[1].wait()
    rows = [spot] + codes + [weight[k:k + 1, :] for k in range(2)] + seats + [spot]
    columns = jnp.transpose(jnp.concatenate(rows, axis=0))
    slots = OFFSETS * SLOTS
    lanes = lax.broadcasted_iota(jnp.int32, (tokens, slots), 1)
    at_home = lanes == columns[:, 0:1].astype(jnp.int32)
    for q in range(4):
        values = jnp.sum(jnp.where(at_home, columns[:, q + 1:q + 2], 0.0), axis=0, keepdims=True)
        for p in range(Z):
            meta_s[p, q:q + 1, :] = values[:, p * Y * SLOTS:(p + 1) * Y * SLOTS]
    repeated = lax.broadcasted_iota(jnp.int32, (tokens, 2 * tokens), 1) % tokens
    repeated = repeated == lax.broadcasted_iota(jnp.int32, (tokens, 2 * tokens), 0)
    for k in range(3):
        values = jnp.where(repeated, columns[:, 5 + k:6 + k], 0.0)
        tables[0, 0, k:k + 1, :] = jnp.sum(values, axis=0, keepdims=True)
    tables[0, 0, 3:4, :] = jnp.zeros((1, 2 * tokens), jnp.float32)
    inputs[2].wait()
    inputs[3].wait()

    pl.semaphore_wait(barrier, len(near))

    def remote(src, dst, send, recv, peer, c):
        return pltpu.make_async_remote_copy(
            src_ref=src, dst_ref=dst, send_sem=send, recv_sem=recv,
            device_id=(peer, c), device_id_type=MESH,
        )

    def arrived(ref, sem):
        pltpu.make_async_copy(ref, ref, sem).wait()

    def pass_on(p, j, q, i, peer):
        remote(tables.at[p, j], tables.at[q, i], s_sem.at[0], table_sem.at[q, i], peer, core).start()
        remote(blocks.at[p, j], blocks.at[q, i], s_sem.at[1], block_sem.at[q, i], peer, core).start()

    up, down = plane(1, 0, 1), plane(1, 0, -1)
    middle = Z // 2

    def step_g(k, j):
        for p in sorted({place_of[k], place_of[(Z - k) % Z]}):
            chunk_here(p, j)
        if (k, j) == (1, 0) and middle > 2:
            return
        if k + 1 < middle or j < X // 2:
            pass_on(place_of[k], j, place_of[k + 1], j, up)
        if k + 1 < middle or j >= X // 2:
            pass_on(place_of[(Z - k) % Z], j, place_of[Z - k - 1], j, down)
        if (k, j) == (0, 0) and middle > 2:
            pass_on(0, 0, place_of[2], 0, plane(2, 0, 1))
            pass_on(0, 0, place_of[Z - 2], 0, plane(2, 0, -1))

    seen = {(0, 0)}

    def chunk_here(p, j):
        if (p, j) not in seen:
            seen.add((p, j))
            arrived(tables.at[p, j], table_sem.at[p, j])
            arrived(blocks.at[p, j], block_sem.at[p, j])

    for dx in GATHER:
        pass_on(0, 0, 0, dx, line(dx, 1))
    step_g(0, 0)
    def step_m(p):
        assert (place_of[(Z - STEPS[p]) % Z], 0) in seen
        for dy in range(Y):
            if p or dy:
                o, peer = p * Y + dy, plane(STEPS[p], dy, 1)
                remote(meta_s.at[p], meta_r.at[o], s_sem.at[2], meta_sem.at[p], peer, core).start()
            else:
                pltpu.make_async_copy(meta_s.at[0], meta_r.at[0], meta_sem.at[0]).start()

    step_m(0)

    gain_copy = remote(gains.at[core], gains.at[core], far_send.at[3], far_recv.at[3], me, other)
    gain_copy.start()
    for copy in give:
        copy.wait()
    far = [
        remote(stage, dst.at[core], far_send.at[i], far_recv.at[i], me, other)
        for i, (_, dst, stage) in enumerate(stores)
    ]
    for copy in far:
        copy.start()

    def codes_of(p):
        segment = lax.broadcasted_iota(jnp.int32, (4, Y * SLOTS), 1) // SLOTS
        table = jnp.zeros((4, Y * SLOTS), jnp.float32)
        for dy in range(Y):
            table = jnp.where(segment == dy, meta_r[p * Y + dy], table)
        return table

    def step_a(p, first, last):
        count = last - first
        for j in range(first, last):
            chunk_here(p, j)
        at = pl.ds(first, count)
        spot_of = lax.broadcasted_iota(jnp.int32, (4, count * tokens), 1) // tokens
        seat = jnp.zeros((4, count * tokens), jnp.float32)
        for j in range(count):
            seat = jnp.where(spot_of == j, tables[p, first + j, :, :count * tokens], seat)
        seat = seat.astype(jnp.int32)
        pick = seat // CAP
        group, expert = pick // EXPERTS, pick % EXPERTS
        dy = (group % Y - y + Y) % Y
        target = ((spot_of * Y + dy) * 2 + expert % 2) * CAP + seat % CAP
        target = jnp.where((group // Y == z) & (expert // 2 == x), target, -1)
        places = lax.broadcasted_iota(jnp.int32, (count * Y * 2 * CAP, count * tokens), 0)
        take = (places == target[0:1]) | (places == target[1:2])
        take = take.astype(jnp.float32).astype(jnp.bfloat16)
        source = blocks[p, first:last].reshape(count * tokens, half)
        chosen = jnp.dot(take, source, preferred_element_type=jnp.float32)
        send_2[p, first:last] = chosen.reshape(count, Y, 2, CAP, half).astype(jnp.bfloat16)
        for dy in COLUMN:
            for c in range(2):
                remote(
                    send_2.at[p, at, dy, c], recv_2.at[core, p, at, dy], s_sem.at[3], sem_2.at[p], plane(0, dy, 1), c
                ).start()
        remote(send_2.at[p, at, 0, other], recv_2.at[core, p, at, 0], s_sem.at[3], sem_2.at[p], me, other).start()
        pltpu.make_async_copy(send_2.at[p, at, 0, core], recv_2.at[core, p, at, 0], sem_2.at[p]).start()

    ready = []

    def step_f(p):
        count = Y * CAP
        at = pl.ds(p * count, count)
        arrived(recv_2.at[:, p], sem_2.at[p])
        if not ready:
            gain_copy.wait()
        parts = [recv_2[h, p].astype(jnp.float32).reshape(X * count, half) for h in range(2)]
        squares = sum(jnp.sum(part * part, axis=1, keepdims=True) for part in parts)
        scale = lax.rsqrt(squares / (2 * half) + EPSILON)
        normed = jnp.concatenate(
            [(part * scale * gains[h]).astype(jnp.bfloat16) for h, part in enumerate(parts)], axis=1
        )
        if not ready:
            for copy in own + far[:2]:
                copy.wait()
        hidden = []
        for h in range(2):
            gate = jnp.dot(normed, wg[h], preferred_element_type=jnp.float32)
            up = jnp.dot(normed, wu[h], preferred_element_type=jnp.float32)
            hidden.append((jax.nn.silu(gate) * up).astype(jnp.bfloat16))
        hidden = jnp.concatenate(hidden, axis=1)
        if not ready:
            far[2].wait()
            ready.append(True)
        for f in range(2):
            result = jnp.dot(hidden, wd[f], preferred_element_type=jnp.float32).astype(jnp.bfloat16)
            send_3[:, f, p * count:(p + 1) * count, :] = result.reshape(X, count, half)
        mine = x * 2 + core
        for dx in LINE:
            peer = line(dx, -1)
            for c in range(2):
                remote(
                    send_3.at[dx, c, at], recv_3.at[mine, at], s_sem.at[4], sem_3.at[p], peer, c
                ).start()
        remote(send_3.at[0, other, at], recv_3.at[mine, at], s_sem.at[4], sem_3.at[p], me, other).start()
        pltpu.make_async_copy(send_3.at[0, core, at], recv_3.at[mine, at], sem_3.at[p]).start()

    def step_c(p):
        arrived(meta_r.at[pl.ds(p * Y, Y)], meta_sem.at[p])
        table = codes_of(p)
        table = jnp.transpose(jnp.concatenate([table, jnp.zeros_like(table)], axis=0))
        block = lax.broadcasted_iota(jnp.int32, (Y * SLOTS, 1), 0) // SLOTS
        places = lax.broadcasted_iota(jnp.int32, (Y * SLOTS, EXPERTS * Y * CAP), 1)
        take = []
        for k in range(2):
            code = table[:, k:k + 1].astype(jnp.int32) - 1
            code = (code >> 3) * (Y * CAP) + block * CAP + (code & 7)
            take.append((places == code).astype(jnp.float32).astype(jnp.bfloat16))
        at = pl.ds(p * Y * CAP, Y * CAP)
        arrived(recv_3.at[:, at], sem_3.at[p])
        source = recv_3[:, p * Y * CAP:(p + 1) * Y * CAP, :].reshape(EXPERTS * Y * CAP, half)
        total = 0.0
        for k in range(2):
            total = total + table[:, 2 + k:3 + k] * jnp.dot(take[k], source, preferred_element_type=jnp.float32)
        send_4[p * Y:(p + 1) * Y] = total.astype(jnp.bfloat16).reshape(Y, SLOTS, half)
        for dy in COLUMN:
            o = p * Y + dy
            remote(send_4.at[o], recv_4.at[o], s_sem.at[5], sem_4.at[p], plane(0, dy, -1), core).start()
        pltpu.make_async_copy(send_4.at[p * Y], recv_4.at[p * Y], sem_4.at[p]).start()

    def step_e(p):
        table = tables[p, 0]
        table = jnp.transpose(jnp.concatenate([table, jnp.zeros_like(table)], axis=0))
        spot = table[:tokens, 2:3].astype(jnp.int32) - p * Y * SLOTS
        places = lax.broadcasted_iota(jnp.int32, (tokens, Y * SLOTS), 1)
        take = (places == spot).astype(jnp.float32).astype(jnp.bfloat16)
        arrived(recv_4.at[pl.ds(p * Y, Y)], sem_4.at[p])
        source = recv_4[p * Y:(p + 1) * Y].reshape(Y * SLOTS, half)
        send_5[p] = jnp.dot(take, source, preferred_element_type=jnp.float32).astype(jnp.bfloat16)
        if p:
            remote(send_5.at[p], recv_5.at[p], s_sem.at[6], sem_5.at[p], plane(STEPS[p], 0, -1), core).start()
        else:
            pltpu.make_async_copy(send_5.at[0], recv_5.at[0], sem_5.at[0]).start()

    sums = []
    last = int(ORDER[-1][1:])

    def step_h(p):
        if p == last:
            sums.append(sum(recv_5[q].astype(jnp.float32) for q in range(Z) if q != last))
        arrived(recv_5.at[p], sem_5.at[p])

    step_of = {"G": step_g, "M": step_m, "A": step_a, "F": step_f, "C": step_c, "E": step_e, "H": step_h}
    for name in ORDER:
        if name not in ("G00", "M0"):
            step_of[name[0]](*map(int, name[1:]))
    out_ref[...] = (sums[0] + recv_5[last].astype(jnp.float32)).astype(jnp.bfloat16)

    for at in ((pl.ds(1, Z - 1),), (0, pl.ds(1, X - 1))):
        arrived(tables.at[at], s_sem.at[0])
        arrived(blocks.at[at], s_sem.at[1])
    arrived(meta_r.at[pl.ds(1, OFFSETS - 1)], s_sem.at[2])
    arrived(recv_2.at[0, :, :, pl.ds(1, Y - 1)], s_sem.at[3])
    arrived(recv_2.at[1], s_sem.at[3])
    arrived(recv_3.at[pl.ds(1, EXPERTS - 1)], s_sem.at[4])
    arrived(send_4.at[pl.ds(0, OFFSETS - Z)], s_sem.at[5])
    arrived(send_5.at[pl.ds(1, Z - 1)], s_sem.at[6])


def solution(mesh):
    assert mesh.shape["ep"] == Z * Y * X and mesh.shape["tp"] == 2

    def local(tokens, norm_gain, routing, route_weight, w_gate, w_up, w_down):
        rows, half = tokens.shape
        vmem = pl.BlockSpec(memory_space=pltpu.VMEM)
        far = pl.BlockSpec(memory_space=pl.ANY)
        dma = pltpu.SemaphoreType.DMA
        bf16, f32 = jnp.bfloat16, jnp.float32
        line_rows = OFFSETS * CAP
        rounds = dma((Z,))
        return pl.pallas_call(
            kernel,
            out_shape=pltpu.VMEM((rows, half), bf16),
            in_specs=[far] * 7,
            out_specs=vmem,
            scratch_shapes=[
                pltpu.VMEM((2, rows), jnp.int32),
                pltpu.VMEM((2, rows), f32),
                pltpu.VMEM((2, 1, half), f32),
                pltpu.VMEM(w_gate.shape, bf16),
                pltpu.VMEM(w_up.shape, bf16),
                pltpu.VMEM(w_down.shape, bf16),
                pltpu.VMEM(w_gate.shape[1:], bf16),
                pltpu.VMEM(w_up.shape[1:], bf16),
                pltpu.VMEM(w_down.shape[1:], bf16),
                pltpu.VMEM((Z, 4, Y * SLOTS), f32),
                pltpu.VMEM((OFFSETS, 4, Y * SLOTS), f32),
                pltpu.VMEM((Z, X, rows, half), bf16),
                pltpu.VMEM((Z, X, 4, 2 * rows), f32),
                pltpu.VMEM((Z, X, Y, 2, CAP, half), bf16),
                pltpu.VMEM((2, Z, X, Y, CAP, half), bf16),
                pltpu.VMEM((X, 2, line_rows, half), bf16),
                pltpu.VMEM((EXPERTS, line_rows, half), bf16),
                pltpu.VMEM((OFFSETS, SLOTS, half), bf16),
                pltpu.VMEM((OFFSETS, SLOTS, half), bf16),
                pltpu.VMEM((Z, rows, half), bf16),
                pltpu.VMEM((Z, rows, half), bf16),
                dma((4,)), dma((3,)), dma((3,)), dma((4,)), dma((4,)), dma((7,)),
                rounds, dma((Z, X)), dma((Z, X)), rounds, rounds, rounds, rounds,
            ],
            compiler_params=pltpu.CompilerParams(collective_id=0, has_side_effects=True),
            name="experts",
        )(tokens, norm_gain.reshape(1, half), routing.T, route_weight.T, w_gate, w_up, w_down)

    in_specs = (
        P("ep", "tp"), P("tp"), P("ep", None), P("ep", None),
        P("ep", None, "tp"), P("ep", None, "tp"), P("ep", None, "tp"),
    )
    return jax.shard_map(local, mesh=mesh, in_specs=in_specs, out_specs=P("ep", "tp"), check_vma=False)
```
